512 devices in a mesh: sp: 128 (over z, x, core), tp: 4 (over y).
Axes of the slice: x: 4, y: 4, z: 16, core: 2. Of those that a mesh axis runs over, the one named last changes fastest.
Arguments:
- queries: bfloat16 [16384, 1024], P('sp', 'tp'), may hold values from -12 to 12
- keys: bfloat16 [16384, 256], P('sp', 'tp'), may hold values from -12 to 12
- values: bfloat16 [16384, 256], P('sp', 'tp'), may hold values from -6 to 6
- log_gate: float32 [16, 16384], P('tp', 'sp'), may hold values from -0.2 to 0, as said below
- log_sum: float32 [16, 16384], P('tp', 'sp'), may hold values from -100 to 100, as said below
- output: bfloat16 [16384, 1024], P('sp', 'tp'), may hold values from -6 to 6
- cotangent: bfloat16 [16384, 1024], P('sp', 'tp'), may hold values from -12 to 12
- normed: bfloat16 [16384, 2048], P('sp', 'tp'), may hold values from -24 to 24
Outputs:
- query_grad: bfloat16 [16384, 1024], P('sp', 'tp')
- key_grad: bfloat16 [16384, 256], P('sp', 'tp')
- value_grad: bfloat16 [16384, 256], P('sp', 'tp')
- weight_grad: float32 [2048, 256], P('sp', 'tp')
The draws below stay inside these ranges and needn't reach their ends.
Inputs may be any that keep to these rules, and one draw needn't show every extreme that they name: `log_gate`: every entry is negative. log_sum[h, t] is the logarithm of the sum over s <= t of exp of the scores of the steps (before log_sum is subtracted), computed from the given queries, keys and log_gate.
All inputs are finite; a program needn't handle non-finite values.
Results may differ from the reference program's by a relative error of at most 0.005.
Values may be sent and summed in bfloat16 or wider, within the bound.
A program may use at most 64 MiB of HBM per device.

```python
import math
import jax
import jax.numpy as jnp
from jax import lax

D = 2048
HEADS = 16
KV_HEADS = 4
HDIM = 64
TOK_DEV = 128
SEQ = 16384


def make_gates(key):
    streams = jax.random.split(jax.random.fold_in(key, 11), 5)
    order = jax.random.permutation(streams[0], HEADS)
    lasting = order < HEADS // 2
    slow_rate = jax.random.uniform(streams[1], (HEADS,), jnp.float32, 0.3, 1.5) / SEQ
    fast_rate = jnp.exp(jax.random.uniform(streams[2], (HEADS,), jnp.float32, math.log(0.01), math.log(1.0 / 30.0)))
    rates = jnp.where(lasting, slow_rate, fast_rate)
    factors = jnp.exp(jax.random.uniform(streams[3], (HEADS, SEQ // TOK_DEV), jnp.float32, -0.7, 0.7))
    factors = jnp.repeat(factors, TOK_DEV, axis=1)
    rough = jax.random.uniform(streams[4], (HEADS, SEQ), jnp.float32, 0.5, 1.5)
    return -rates[:, None] * factors * rough


def make_queries(key):
    drawn = jax.random.normal(jax.random.fold_in(key, 21), (SEQ, HEADS * HDIM), jnp.float32)
    return jnp.clip(drawn, -12.0, 12.0).astype(jnp.bfloat16)


def make_keys(key):
    drawn = jax.random.normal(jax.random.fold_in(key, 31), (SEQ, KV_HEADS * HDIM), jnp.float32)
    return jnp.clip(drawn, -12.0, 12.0).astype(jnp.bfloat16)


def draw_queries(key, part):
    return make_queries(key)


def draw_keys(key, part):
    return make_keys(key)


def draw_log_gate(key, part):
    return make_gates(key)


def draw_log_sum(key, part):
    group_size = HEADS // KV_HEADS
    block_count = SEQ // TOK_DEV
    inverse_root = HDIM ** (-0.5)
    query_float = make_queries(key).astype(jnp.float32).reshape(block_count, TOK_DEV, KV_HEADS, group_size, HDIM)
    query_float = jnp.transpose(query_float, (2, 0, 1, 3, 4))
    key_float = jnp.transpose(make_keys(key).astype(jnp.float32).reshape(SEQ, KV_HEADS, HDIM), (1, 0, 2))
    cumulative = jnp.cumsum(make_gates(key), axis=1)
    cum_blocks = jnp.transpose(cumulative.reshape(KV_HEADS, group_size, block_count, TOK_DEV), (0, 2, 1, 3))
    cum_keys = cumulative.reshape(KV_HEADS, group_size, SEQ)
    key_positions = jnp.arange(SEQ)

    def one_group(inputs):
        query_group, cum_group, key_group, key_cum = inputs

        def one_block(pieces):
            query_block, cum_block, block_index = pieces
            query_positions = block_index * TOK_DEV + jnp.arange(TOK_DEV)
            scores = jnp.einsum('qgd,kd->gqk', query_block, key_group, precision=lax.Precision.HIGHEST) * inverse_root
            scores = scores + cum_block[:, :, None] - key_cum[:, None, :]
            allowed = key_positions[None, :] <= query_positions[:, None]
            scores = jnp.where(allowed[None], scores, -jnp.inf)
            return jax.nn.logsumexp(scores, axis=2)
        return lax.map(one_block, (query_group, cum_group, jnp.arange(block_count)))
    sums = lax.map(one_group, (query_float, cum_blocks, key_float, cum_keys))
    return jnp.transpose(sums, (0, 2, 1, 3)).reshape(HEADS, SEQ)


def spiked(values, rng, source, target, blocks, factor):
    owner, partner = [(jnp.arange(values.shape[position]) // (values.shape[position] // blocks)).reshape([-1 if axis == position else 1 for axis in range(values.ndim)]) for position in (source, target)]
    chosen = jax.random.permutation(rng, blocks)[partner]
    strong = (owner == chosen) | (owner == (partner + blocks // 2) % blocks)
    return jnp.where(strong, factor * values, values)


def shard_levels(key, dims, cuts, low, high):
    def one(axis_at, shards_of):
        draws = jax.random.uniform(jax.random.fold_in(jax.random.fold_in(key, 6), axis_at), (shards_of,), jnp.float32, low / len(cuts), high / len(cuts))
        return jnp.repeat(jnp.exp(draws), dims[axis_at] // shards_of).reshape((-1,) + (1,) * (len(dims) - axis_at - 1))

    loudness = one(*cuts[0])
    for cut in cuts[1:]:
        loudness = loudness * one(*cut)
    return loudness


def scatter_about(own_key, shape, spread, bound, cuts=(), kind=jnp.bfloat16):
    loudness = shard_levels(own_key, shape, cuts, -0.22, 0.18) if cuts else 1.0
    values = jax.random.normal(own_key, shape, jnp.float32) * spread * loudness
    return jnp.minimum(jnp.maximum(values, -bound), bound).astype(kind)


def noise_with(own_key, shape, spread, limit, cuts, heavy, dtype=jnp.bfloat16):
    values = spread * jax.random.normal(own_key, shape, jnp.float32)
    if cuts:
        values = values * shard_levels(own_key, shape, cuts, -0.22, 0.18)
    return jnp.clip(spiked(values, jax.random.fold_in(own_key, 3), *heavy), -limit, limit).astype(dtype)


def setup_inputs(seed: int = 0) -> dict:
    streams_of = jax.random.split(jax.random.key(seed), 9)
    return {
        "queries": draw_queries(jax.random.fold_in(streams_of[8], 71), 0),
        "keys": draw_keys(jax.random.fold_in(streams_of[8], 71), 0),
        "values": scatter_about(streams_of[2], (SEQ, KV_HEADS * HDIM), 1.0, 6.0, ((0, 128), (1, 4))),
        "log_gate": draw_log_gate(jax.random.fold_in(streams_of[8], 71), 0),
        "log_sum": draw_log_sum(jax.random.fold_in(streams_of[8], 71), 0),
        "output": scatter_about(streams_of[5], (SEQ, HEADS * HDIM), 1.0, 6.0, ((0, 128), (1, 4))),
        "cotangent": scatter_about(streams_of[6], (SEQ, HEADS * HDIM), 2.0, 12.0, ((0, 128), (1, 4))),
        "normed": noise_with(streams_of[7], (SEQ, D), 1.0, 24.0, ((0, 128), (1, 4)), (0, 1, 128, 5.5)),
    }


NEG_LARGE = -1e30


def to_low(array):
    rounded = lax.optimization_barrier(array.astype(jnp.bfloat16))
    return rounded.astype(jnp.float32)


def reference(queries, keys, values, log_gate, log_sum, output, cotangent, normed):
    group_size = HEADS // KV_HEADS
    block_count = SEQ // TOK_DEV
    inverse_root = HDIM ** -0.5
    cumulative = jnp.cumsum(log_gate, axis=1)
    row_terms = jnp.sum((output.astype(jnp.float32) * cotangent.astype(jnp.float32)).reshape(SEQ, HEADS, HDIM), axis=2).T

    def by_group(array):
        return jnp.transpose(array.reshape(block_count, TOK_DEV, KV_HEADS, group_size, HDIM), (2, 0, 1, 3, 4))

    def rows_group(array):
        return jnp.transpose(array.reshape(KV_HEADS, group_size, block_count, TOK_DEV), (0, 2, 1, 3))

    query_blocks = by_group(queries)
    cotan_blocks = by_group(cotangent)
    cum_blocks = rows_group(cumulative)
    lse_blocks = rows_group(log_sum)
    term_blocks = rows_group(row_terms)
    key_heads = jnp.transpose(keys.reshape(SEQ, KV_HEADS, HDIM), (1, 0, 2))
    value_heads = jnp.transpose(values.reshape(SEQ, KV_HEADS, HDIM), (1, 0, 2))
    cum_keys = cumulative.reshape(KV_HEADS, group_size, SEQ)
    key_positions = jnp.arange(SEQ)

    def one_group(inputs):
        query_group, cotan_group, cum_group, lse_group, term_group, key_group, value_group, key_cum = inputs
        key_float = key_group.astype(jnp.float32)
        value_float = value_group.astype(jnp.float32)

        def one_block(state_now, pieces):
            key_total, value_total = state_now
            query_block, cotan_block, cum_block, lse_block, term_block, block_index = pieces
            query_positions = block_index * TOK_DEV + jnp.arange(TOK_DEV)
            query_float = query_block.astype(jnp.float32)
            cotan_float = cotan_block.astype(jnp.float32)
            scores = jnp.einsum("qgd,kd->gqk", query_float, key_float) * inverse_root
            scores = scores + cum_block[:, :, None] - key_cum[:, None, :] - lse_block[:, :, None]
            allowed = key_positions[None, :] <= query_positions[:, None]
            weights = jnp.exp(jnp.where(allowed[None], scores, NEG_LARGE))
            upstream = jnp.einsum("qgd,kd->gqk", cotan_float, value_float)
            dscore = weights * (upstream - term_block[:, :, None])
            weights_low = to_low(weights)
            dscore_low = to_low(dscore)
            query_part = jnp.einsum("gqk,kd->qgd", dscore_low, key_float) * inverse_root
            key_total = key_total + jnp.einsum("gqk,qgd->kd", dscore_low, query_float) * inverse_root
            value_total = value_total + jnp.einsum("gqk,qgd->kd", weights_low, cotan_float)
            return (key_total, value_total), query_part

        zeros_start = jnp.zeros((SEQ, HDIM), jnp.float32)
        totals, query_parts = lax.scan(one_block, (zeros_start, zeros_start),
                                       (query_group, cotan_group, cum_group, lse_group, term_group,
                                        jnp.arange(block_count)))
        return query_parts, totals[0], totals[1]

    query_parts, key_parts, value_parts = lax.map(one_group, (query_blocks, cotan_blocks, cum_blocks, lse_blocks,
                                                              term_blocks, key_heads, value_heads, cum_keys))
    query_grad = jnp.transpose(query_parts, (1, 2, 0, 3, 4)).reshape(SEQ, HEADS * HDIM).astype(jnp.bfloat16)
    key_grad = jnp.transpose(key_parts, (1, 0, 2)).reshape(SEQ, KV_HEADS * HDIM).astype(jnp.bfloat16)
    value_grad = jnp.transpose(value_parts, (1, 0, 2)).reshape(SEQ, KV_HEADS * HDIM).astype(jnp.bfloat16)
    weight_grad = jnp.dot(normed.T, key_grad, preferred_element_type=jnp.float32)
    return (query_grad, key_grad, value_grad, weight_grad)
```

```python
import functools
import math

import jax
import jax.numpy as jnp
from jax import lax
from jax.experimental import pallas as pl
from jax.experimental.pallas import tpu as pltpu
from jax.sharding import Mesh
from jax.sharding import PartitionSpec as P

SP = ("sp_0", "sp_1", "sp_2")
MESH = pl.DeviceIdType.MESH
LOG2E = math.log2(math.e)
NEG_LARGE = -1e30
TOK = 128
TQ = 256
F32, BF16 = jnp.float32, jnp.bfloat16


def at(z=None, x=None, c=None, y=None):
    named = {"sp_0": z, "sp_1": x, "sp_2": c, "tp": y}
    return {k: v for k, v in named.items() if v is not None}


def greet(peers):
    barrier = pltpu.get_barrier_semaphore()
    for peer in peers:
        pl.semaphore_signal(barrier, inc=1, device_id=peer, device_id_type=MESH)
    pl.semaphore_wait(barrier, len(peers))


def remote(src, dst, send, recv, peer):
    return pltpu.make_async_remote_copy(
        src_ref=src, dst_ref=dst, send_sem=send, recv_sem=recv, device_id=peer, device_id_type=MESH
    )


def attention_kernel(
    nz, nx, ny,
    q_ref, k_ref, gate_ref, lse_ref, out_ref, do_ref, norm_ref,
    dq_out, dkv_out, norm_out,
    qg, dg, kv, aux, stat, kaux, ck, rowb, qtl, dtl, ktile, vtile, kcat, dq, dkvt, own,
    gsend, grecv, dqd, dqs, dqr,
    aux_s, aux_r, q_s, q_r, f_s, k_s, k_r, ka_s, ka_r, n_s, n_r, g_s, g_r, d_s, d_r, e_s, e_r,
):
    z, x, c, y = (lax.axis_index(a) for a in ("sp_0", "sp_1", "sp_2", "tp"))
    nb = 2 * nx
    b = 2 * x + c
    sib = at(c=1 - c)
    c1 = 0.125 * LOG2E

    def xc(r):
        k = lax.rem(b + r, nb)
        return at(x=k // 2, c=lax.rem(k, 2))

    def zz(r):
        return at(z=lax.rem(z + r, nz))

    def yy(r):
        return at(y=lax.rem(y + r, ny))

    gates = gate_ref[...]
    lane = lax.broadcasted_iota(jnp.int32, (4, TOK), 1)
    run = gates
    for s in (1, 2, 4, 8, 16, 32, 64):
        run = run + jnp.where(lane >= s, pltpu.roll(run, s, 1), 0.0)
    prod = (out_ref[...].astype(F32) * do_ref[...].astype(F32)).T
    terms = jnp.sum(prod.reshape(4, 64, TOK), axis=1)
    aux[b, 0:4, :] = run
    aux[b, 4:8, :] = run - lse_ref[...]
    aux[b, 8:12, :] = terms
    aux[b, 12:16, :] = jnp.zeros((4, TOK), F32)
    qg[b] = q_ref[...]
    dg[b] = do_ref[...]
    kv[z] = k_ref[...]

    greet([xc(r) for r in range(1, nb)] + [zz(r) for r in range(1, nz)] + [yy(r) for r in range(1, ny)])

    for r in range(1, nb):
        remote(aux.at[b], aux.at[b], aux_s.at[r], aux_r.at[b], xc(r)).start()
    for i, (src, dst) in enumerate(((q_ref, qg), (do_ref, dg))):
        remote(src, dst.at[b], f_s.at[i, x], q_r.at[i, b], sib).start()
    xorder = [r for pair in zip(range(1, nx // 2 + 1), range(nx - 1, nx // 2 - 1, -1)) for r in pair]
    xorder = list(dict.fromkeys(xorder))
    for r in xorder:
        peer = lax.rem(x + r, nx)
        for i, (src, dst) in enumerate(((q_ref, qg), (do_ref, dg))):
            remote(src, dst.at[b], q_s.at[i, r], q_r.at[i, b], at(x=peer)).start()
    zorder = [r for pair in zip(range(1, nz // 2 + 1), range(nz - 1, nz // 2 - 1, -1)) for r in pair]
    zorder = list(dict.fromkeys(zorder))

    def k_copy(r, peer):
        return remote(k_ref, kv.at[z], k_s.at[r], k_r.at[z], at(z=peer))

    def ka_copy(r, peer):
        return remote(kaux.at[z], kaux.at[z], ka_s.at[r], ka_r.at[z], at(z=peer))

    for r in zorder:
        peer = lax.rem(z + r, nz)

        @pl.when(peer > z)
        def _():
            k_copy(r, peer).start()

    for r in range(1, ny):
        remote(norm_ref, norm_out.at[y], n_s.at[r], n_r.at[y], yy(r)).start()
    norm_out[y] = norm_ref[...]

    for r in range(1, nb):
        k = lax.rem(b + r, nb)
        remote(aux.at[k], aux.at[k], aux_s.at[r], aux_r.at[k], xc(r)).wait_recv()
    before = jnp.zeros((4, TOK), F32)
    mine = jnp.zeros((4, TOK), F32)
    for k in range(nb):
        mine = jnp.where(b == k, before, mine)
        stat[k, 0:4, :] = (aux[k, 4:8, :] + before) * LOG2E
        stat[k, 4:8, :] = aux[k, 8:12, :]
        before = before + jnp.broadcast_to(aux[k, 0:4, TOK - 1 : TOK], (4, TOK))
    kaux[z, 0:4, :] = run + mine
    kaux[z, 4:8, :] = before

    for r in zorder:
        peer = lax.rem(z + r, nz)

        @pl.when(peer > z)
        def _():
            ka_copy(r, peer).start()

    for r in xorder:
        k = 2 * lax.rem(x + nx - r, nx) + c
        for i, dst in enumerate((qg, dg)):
            remote(dst.at[k], dst.at[k], q_s.at[i, 0], q_r.at[i, k], sib).wait_recv()
            remote(dst.at[k], dst.at[k], f_s.at[i, lax.rem(x + nx - r, nx)], q_r.at[i, k], sib).start()

    def offsets(i, total):
        k = z - 1 - i
        remote(kaux.at[k], kaux.at[k], ka_s.at[0], ka_r.at[k], sib).wait_recv()
        total = total + kaux[k, 4:8, :]
        ck[k, 0:4, :] = (kaux[k, 0:4, :] - total) * LOG2E
        return total

    ck[z, 0:4, :] = (run + mine) * LOG2E
    lax.fori_loop(0, z, offsets, jnp.zeros((4, TOK), F32))

    for k in range(nx):
        slot = 2 * k + 1 - c
        for i, dst in enumerate((qg, dg)):
            remote(dst.at[slot], dst.at[slot], q_s.at[i, 0], q_r.at[i, slot], sib).wait_recv()

    tb = TQ // TOK
    nt = nb // tb

    def prepare(k, _):
        t, i = k // tb, lax.rem(k, tb)
        qt = qg[k].T
        dt = dg[k].T
        stats = jnp.concatenate([stat[k], jnp.zeros((TOK - 8, TOK), F32)], 0).T
        for h in range(4):
            for j in range(tb):
                @pl.when(i == j)
                def _():
                    qtl[t, :, h * TQ + j * TOK : h * TQ + (j + 1) * TOK] = qt[64 * h : 64 * h + 64]
                    dtl[t, :, h * TQ + j * TOK : h * TQ + (j + 1) * TOK] = dt[64 * h : 64 * h + 64]
        for r in range(8):
            rowb[r, k] = jnp.broadcast_to(stats[:, r : r + 1], (TOK, TOK))
        dq[k] = jnp.zeros((TOK, 256), F32)
        return 0

    lax.fori_loop(0, nb, prepare, 0)

    even = lax.rem(z, 2) == 1
    skip = jnp.where(even, 0, 1)
    straight = jnp.minimum(nz - 1 - z, z)
    lane2 = lax.broadcasted_iota(jnp.int32, (TOK, TOK), 1)
    zero = jnp.zeros((64, TOK), BF16)

    def visit(s):
        t = s - straight
        far = jnp.where(lax.rem(t, 2) == 1, z - straight - (t + 1) // 2, t // 2 - 1)
        return jnp.where(s <= straight, z - s, far)

    def load_keys(blocks):
        for i, k in enumerate(blocks):
            block = kv[k]
            t = block.T
            cols = slice(i * TOK, (i + 1) * TOK)
            ktile[0, :, cols] = jnp.concatenate([t[:64], zero], 0)
            ktile[1, :, cols] = jnp.concatenate([zero, t[:64]], 0)
            vtile[0, :, cols] = jnp.concatenate([t[64:], zero], 0)
            vtile[1, :, cols] = jnp.concatenate([zero, t[64:]], 0)
            rolled = pltpu.roll(block.astype(F32), 64, 1).astype(BF16)
            none = jnp.zeros_like(block)
            kcat[i * TOK : (i + 1) * TOK, :] = jnp.where(lane2 < 64, block, none)
            kcat[2 * TOK + i * TOK : 2 * TOK + (i + 1) * TOK, :] = jnp.where(lane2 >= 64, rolled, none)

    def run_tile(blocks, first):
        load_keys(blocks)
        dkvt[...] = jnp.zeros((TOK, 2 * TOK), F32)
        cks = [jnp.concatenate([ck[k, h : h + 1, :] for k in blocks], 1) for h in range(4)]
        if first:
            col = lax.broadcasted_iota(jnp.int32, (TQ, 2 * TOK), 1)
            other = jnp.where(even, -1, 1 << 20)
            key_pos = jnp.where(col < TOK, b * TOK + col, other)

        def rows(t, _):
            q = qg[pl.ds(tb * t, tb)].reshape(TQ, 256)
            do = dg[pl.ds(tb * t, tb)].reshape(TQ, 256)
            ps, dss = [], []
            if first:
                allowed = key_pos <= lax.broadcasted_iota(jnp.int32, (TQ, 2 * TOK), 0) + t * TQ
            for h in range(4):
                lanes = slice(128 * (h // 2), 128 * (h // 2) + 128)
                s = jnp.dot(q[:, lanes], ktile[h % 2], preferred_element_type=F32)
                ra = rowb[h, pl.ds(tb * t, tb)].reshape(TQ, TOK)
                rd = rowb[4 + h, pl.ds(tb * t, tb)].reshape(TQ, TOK)
                logits = (s * c1 + jnp.concatenate([ra, ra], 1)) - cks[h]
                if first:
                    logits = jnp.where(allowed, logits, NEG_LARGE)
                p = jnp.exp2(logits)
                dp = jnp.dot(do[:, lanes], vtile[h % 2], preferred_element_type=F32)
                ds = p * (dp - jnp.concatenate([rd, rd], 1))
                ps.append(p.astype(BF16))
                dss.append(ds.astype(BF16))
            dkvt[:64] += jnp.dot(qtl[t], jnp.concatenate(dss, 0), preferred_element_type=F32)
            dkvt[64:] += jnp.dot(dtl[t], jnp.concatenate(ps, 0), preferred_element_type=F32)
            for g in range(2):
                pair = jnp.concatenate([dss[2 * g], dss[2 * g + 1]], 1)
                add = jnp.dot(pair, kcat[...], preferred_element_type=F32)
                dq[pl.ds(tb * t, tb), :, 128 * g : 128 * g + 128] += add.reshape(tb, TOK, TOK)
            return 0

        lax.fori_loop(0, nt, rows, 0)

    def wait_keys(k):
        remote(kv.at[k], kv.at[k], k_s.at[0], k_r.at[k], sib).wait_recv()

    def g_copy(k):
        return remote(gsend.at[k], grecv.at[z], g_s.at[k], g_r.at[z], at(z=k))

    def pass_on(i, k):
        gsend[k] = dkvt[:, i * TOK : (i + 1) * TOK].T.astype(BF16)
        g_copy(k).start()

    second = jnp.where(even, visit(1), z)

    @pl.when(even)
    def _():
        wait_keys(second)

    run_tile((z, second), True)
    own[...] = dkvt[:, :TOK].T

    @pl.when(even)
    def _():
        pass_on(1, second)

    def later(i, _):
        blocks = (visit(2 * i - skip), visit(2 * i + 1 - skip))
        for k in blocks:
            wait_keys(k)
        run_tile(blocks, False)
        for j, k in enumerate(blocks):
            pass_on(j, k)
        return 0

    lax.fori_loop(1, (z + 2) // 2, later, 0)

    for r in xorder + [0]:
        k = lax.rem(x + r, nx)
        slot = 2 * k + 1 - c
        remote(dq.at[slot], dqd.at[k], d_s.at[k], d_r.at[k], sib).start()
    for r in xorder:
        k = lax.rem(x + r, nx)
        remote(dqd.at[k], dqd.at[k], d_s.at[k], d_r.at[k], sib).wait_recv()
        dqs[k] = ((dq[2 * k + c] + dqd[k]) * 0.125).astype(BF16)
        remote(dqs.at[k], dqr.at[x], e_s.at[k], e_r.at[x], at(x=k)).start()
    remote(dqd.at[x], dqd.at[x], d_s.at[x], d_r.at[x], sib).wait_recv()
    total = (dq[b] + dqd[x]) * 0.125

    def collect(k, _):
        remote(grecv.at[k], grecv.at[k], g_s.at[0], g_r.at[k], sib).wait_recv()
        own[...] += grecv[k].astype(F32)
        return 0

    lax.fori_loop(z + 1, nz, collect, 0)
    scale = jnp.where(lane2 < 64, 0.125, 1.0)
    dkv_out[...] = (own[...] * scale).astype(BF16)

    for r in xorder:
        k = lax.rem(x + r, nx)
        remote(dqr.at[k], dqr.at[k], e_s.at[k], e_r.at[k], sib).wait_recv()
        total = total + dqr[k].astype(F32)
    dq_out[...] = total.astype(BF16)

    for r in range(1, ny):
        k = lax.rem(y + r, ny)
        remote(norm_out.at[k], norm_out.at[k], n_s.at[r], n_r.at[k], sib).wait_recv()

    for r in range(1, nb):
        remote(aux.at[b], aux.at[b], aux_s.at[r], aux_r.at[b], xc(r)).wait_send()
    for i in range(2):
        for k in range(nx):
            remote(q_ref, qg.at[b], f_s.at[i, k], q_r.at[i, b], sib).wait_send()
        for r in range(1, nx):
            remote(q_ref, qg.at[b], q_s.at[i, r], q_r.at[i, b], sib).wait_send()
    for r in range(1, ny):
        remote(norm_ref, norm_out.at[y], n_s.at[r], n_r.at[y], yy(r)).wait_send()
    for r in zorder:
        peer = lax.rem(z + r, nz)

        @pl.when(peer > z)
        def _():
            k_copy(r, peer).wait_send()
            ka_copy(r, peer).wait_send()

    def sent(k, _):
        g_copy(k).wait_send()
        return 0

    lax.fori_loop(0, z, sent, 0)
    for k in range(nx):
        remote(dq.at[0], dqd.at[k], d_s.at[k], d_r.at[k], sib).wait_send()
    for r in range(1, nx):
        k = lax.rem(x + r, nx)
        remote(dqs.at[k], dqr.at[x], e_s.at[k], e_r.at[x], at(x=k)).wait_send()


def attention(nz, nx, ny, q, k, gate, lse, out, do, norm):
    nb = 2 * nx
    vmem = pl.BlockSpec(memory_space=pltpu.VMEM)
    dma = pltpu.SemaphoreType.DMA
    nt = nb * TOK // TQ
    width = norm.shape[1]
    scratch = [
        pltpu.VMEM((nb, TOK, 256), BF16),
        pltpu.VMEM((nb, TOK, 256), BF16),
        pltpu.VMEM((nz, TOK, TOK), BF16),
        pltpu.VMEM((nb, 16, TOK), F32),
        pltpu.VMEM((nb, 8, TOK), F32),
        pltpu.VMEM((nz, 8, TOK), F32),
        pltpu.VMEM((nz, 8, TOK), F32),
        pltpu.VMEM((8, nb, TOK, TOK), F32),
        pltpu.VMEM((nt, 64, 4 * TQ), BF16),
        pltpu.VMEM((nt, 64, 4 * TQ), BF16),
        pltpu.VMEM((2, TOK, 2 * TOK), BF16),
        pltpu.VMEM((2, TOK, 2 * TOK), BF16),
        pltpu.VMEM((4 * TOK, TOK), BF16),
        pltpu.VMEM((nb, TOK, 256), F32),
        pltpu.VMEM((TOK, 2 * TOK), F32),
        pltpu.VMEM((TOK, TOK), F32),
        pltpu.VMEM((nz, TOK, TOK), BF16),
        pltpu.VMEM((nz, TOK, TOK), BF16),
        pltpu.VMEM((nx, TOK, 256), F32),
        pltpu.VMEM((nx, TOK, 256), BF16),
        pltpu.VMEM((nx, TOK, 256), BF16),
        dma((nb,)), dma((nb,)),
        dma((2, nx)), dma((2, nb)), dma((2, nx)),
        dma((nz,)), dma((nz,)), dma((nz,)), dma((nz,)),
        dma((ny,)), dma((ny,)),
        dma((nz,)), dma((nz,)),
        dma((nx,)), dma((nx,)), dma((nx,)), dma((nx,)),
    ]
    return pl.pallas_call(
        functools.partial(attention_kernel, nz, nx, ny),
        out_shape=(
            jax.ShapeDtypeStruct((TOK, 256), BF16),
            jax.ShapeDtypeStruct((TOK, TOK), BF16),
            jax.ShapeDtypeStruct((ny, TOK, width), BF16),
        ),
        in_specs=[vmem] * 7,
        out_specs=(vmem, vmem, vmem),
        scratch_shapes=scratch,
        compiler_params=pltpu.CompilerParams(
            collective_id=0, has_side_effects=True, vmem_limit_bytes=48 * 1024 * 1024
        ),
        name="attention",
    )(q, k, gate, lse, out, do, norm)


def weight_kernel(nz, nx, ny, norm_ref, kg_ref, w_out, part, half, hrecv, mid, msend, mrecv, last, lrecv,
                  h_s, h_r, m_s, m_r, l_s, l_r):
    z, x, c = (lax.axis_index(a) for a in SP)
    sib = at(c=1 - c)
    width = norm_ref.shape[2]
    rows = ny * width // (2 * nx * nz)

    peers = [sib] + [at(x=lax.rem(x + r, nx)) for r in range(1, nx)]
    peers += [at(z=lax.rem(z + r, nz)) for r in range(1, nz)]

    kg = kg_ref[...]
    per = nx * rows * 2
    for k in range(ny):
        w = jnp.dot(norm_ref[k].T, kg, preferred_element_type=F32)
        zs = width // per
        w = w.reshape(zs, nx, 2, rows, 64)
        for cc in range(2):
            part[cc, :, k * zs : (k + 1) * zs] = jnp.swapaxes(w[:, :, cc], 0, 1)
    greet(peers)

    remote(part.at[1 - c], hrecv, h_s, h_r, sib).start()
    remote(part.at[1 - c], hrecv, h_s, h_r, sib).wait_recv()
    order = [r for r in range(1, nx)]
    for r in order:
        k = lax.rem(x + r, nx)
        msend[k] = part[c, k] + hrecv[k]
        remote(msend.at[k], mrecv.at[x], m_s.at[k], m_r.at[x], at(x=k)).start()
    mid[...] = part[c, x] + hrecv[x]
    for r in order:
        k = lax.rem(x + r, nx)
        remote(mrecv.at[k], mrecv.at[k], m_s.at[k], m_r.at[k], sib).wait_recv()
        mid[...] += mrecv[k]
    for r in range(1, nz):
        k = lax.rem(z + r, nz)
        remote(mid.at[k], lrecv.at[z], l_s.at[k], l_r.at[z], at(z=k)).start()
    total = mid[z]
    for r in range(1, nz):
        k = lax.rem(z + r, nz)
        remote(lrecv.at[k], lrecv.at[k], l_s.at[k], l_r.at[k], sib).wait_recv()
        total = total + lrecv[k]
    w_out[...] = total

    remote(part.at[1 - c], hrecv, h_s, h_r, sib).wait_send()
    for r in order:
        k = lax.rem(x + r, nx)
        remote(msend.at[k], mrecv.at[x], m_s.at[k], m_r.at[x], at(x=k)).wait_send()
    for r in range(1, nz):
        k = lax.rem(z + r, nz)
        remote(mid.at[k], lrecv.at[z], l_s.at[k], l_r.at[z], at(z=k)).wait_send()


def weight(nz, nx, ny, norm, kg):
    vmem = pl.BlockSpec(memory_space=pltpu.VMEM)
    dma = pltpu.SemaphoreType.DMA
    rows = ny * norm.shape[2] // (2 * nx * nz)
    return pl.pallas_call(
        functools.partial(weight_kernel, nz, nx, ny),
        out_shape=jax.ShapeDtypeStruct((rows, 64), F32),
        in_specs=[vmem] * 2,
        out_specs=vmem,
        scratch_shapes=[
            pltpu.VMEM((2, nx, nz, rows, 64), F32),
            pltpu.VMEM((8, 128), F32),
            pltpu.VMEM((nx, nz, rows, 64), F32),
            pltpu.VMEM((nz, rows, 64), F32),
            pltpu.VMEM((nx, nz, rows, 64), F32),
            pltpu.VMEM((nx, nz, rows, 64), F32),
            pltpu.VMEM((8, 128), F32),
            pltpu.VMEM((nz, rows, 64), F32),
            dma, dma,
            dma((nx,)), dma((nx,)),
            dma((nz,)), dma((nz,)),
        ],
        compiler_params=pltpu.CompilerParams(
            collective_id=1, has_side_effects=True, vmem_limit_bytes=32 * 1024 * 1024
        ),
        name="weight",
    )(norm, kg)


def body(nz, nx, ny, queries, keys, values, log_gate, log_sum, output, cotangent, normed):
    stacked = jnp.concatenate([keys, values], axis=1)
    query_grad, pair, rows = attention(nz, nx, ny, queries, stacked, log_gate, log_sum, output, cotangent, normed)
    key_grad, value_grad = pair[:, :64], pair[:, 64:]
    weight_grad = weight(nz, nx, ny, rows, key_grad)
    return (query_grad, key_grad, value_grad, weight_grad)


def solution(mesh):
    nz, nx, ny = mesh.shape["sp"] // 8, 4, mesh.shape["tp"]
    split = Mesh(mesh.devices.reshape(nz, nx, 2, ny), SP + ("tp",))
    placed = (
        P(SP, "tp"), P(SP, "tp"), P(SP, "tp"), P("tp", SP),
        P("tp", SP), P(SP, "tp"), P(SP, "tp"), P(SP, "tp"),
    )
    return jax.shard_map(
        functools.partial(body, nz, nx, ny),
        mesh=split,
        in_specs=placed,
        out_specs=(P(SP, "tp"), P(SP, "tp"), P(SP, "tp"), P(SP, "tp")),
        check_vma=False,
    )
```

```python
import functools
import math

import jax
import jax.numpy as jnp
from jax import lax
from jax.experimental import pallas as pl
from jax.experimental.pallas import tpu as pltpu
from jax.sharding import Mesh
from jax.sharding import PartitionSpec as P

SP = ("sp_0", "sp_1", "sp_2")
MESH = pl.DeviceIdType.MESH
LOG2E = math.log2(math.e)
NEG_LARGE = -1e30
TOK = 128
TQ = 256
F32, BF16 = jnp.float32, jnp.bfloat16


def at(z=None, x=None, c=None, y=None):
    named = {"sp_0": z, "sp_1": x, "sp_2": c, "tp": y}
    return {k: v for k, v in named.items() if v is not None}


def remote(src, dst, send, recv, peer):
    return pltpu.make_async_remote_copy(
        src_ref=src, dst_ref=dst, send_sem=send, recv_sem=recv, device_id=peer, device_id_type=MESH
    )


def attention_kernel(
    nz, nx, ny,
    q_in, k_in, v_in, gate_in, lse_in, out_in, do_in, norm_in,
    dq_out, k_out, v_out, w_out,
    q_ref, k_half, v_half, gate_ref, lse_ref, out_ref, do_ref, norm_ref, k_ref,
    qg, dg, kv, aux, stat, kaux, ck, rowb, qtl, dtl, ktile, vtile, kcat, dq, dkvt, own,
    gsend, grecv, dqd, dqs, dqr, norm_all, part, hrecv, msend, mrecv, mid, lrecv,
    i_s, aux_s, aux_r, q_s, q_r, f_s, k_s, k_r, ka_s, ka_r, n_s, n_r, g_s, g_r, d_s, d_r, e_s, e_r,
    h_s, h_r, m_s, m_r, l_s, l_r,
):
    z, x, c, y = (lax.axis_index(a) for a in ("sp_0", "sp_1", "sp_2", "tp"))
    nb = 2 * nx
    b = 2 * x + c
    sib = at(c=1 - c)
    c1 = 0.125 * LOG2E
    tb = TQ // TOK
    nt = nb // tb

    def xc(r):
        k = lax.rem(b + r, nb)
        return at(x=k // 2, c=lax.rem(k, 2))

    def zz(r):
        return at(z=lax.rem(z + r, nz))

    def yy(r):
        return at(y=lax.rem(y + r, ny))

    loads = [
        pltpu.make_async_copy(src, dst, i_s.at[i])
        for i, (src, dst) in enumerate((
            (gate_in, gate_ref), (lse_in, lse_ref), (out_in, out_ref), (do_in, do_ref),
            (k_in, k_half), (v_in, v_half), (q_in, q_ref), (norm_in, norm_ref),
        ))
    ]
    for load in loads:
        load.start()
    peers = [xc(r) for r in range(1, nb)] + [zz(r) for r in range(1, nz)] + [yy(r) for r in range(1, ny)]
    barrier = pltpu.get_barrier_semaphore()
    for peer in peers:
        pl.semaphore_signal(barrier, inc=1, device_id=peer, device_id_type=MESH)
    for load in loads:
        load.wait()

    lane = lax.broadcasted_iota(jnp.int32, (4, TOK), 1)
    run = gate_ref[...]
    for s in (1, 2, 4, 8, 16, 32, 64):
        run = run + jnp.where(lane >= s, pltpu.roll(run, s, 1), 0.0)
    prod = (out_ref[...].astype(F32) * do_ref[...].astype(F32)).T
    aux[b, 0:4, :] = run
    aux[b, 4:8, :] = run - lse_ref[...]
    aux[b, 8:12, :] = jnp.sum(prod.reshape(4, 64, TOK), axis=1)
    aux[b, 12:16, :] = jnp.zeros((4, TOK), F32)
    k_ref[...] = jnp.concatenate([k_half[...], v_half[...]], axis=0).T
    kv[z] = k_ref[...]
    qg[b] = q_ref[...]
    dg[b] = do_ref[...]
    norm_all[y] = norm_ref[...]

    pl.semaphore_wait(barrier, len(peers))

    def nearest_first(n):
        pairs = zip(range(1, n // 2 + 1), range(n - 1, n // 2 - 1, -1))
        return list(dict.fromkeys(r for pair in pairs for r in pair))

    xorder, zorder = nearest_first(nx), nearest_first(nz)
    sources = ((q_ref, qg), (do_ref, dg))

    up, down = nz // 2, nz - 1 - nz // 2

    def reach(stage):
        if stage == 0:
            return [(0, d) for d in (1, 2) if d <= up] + [(0, -d) for d in (1, 2) if d <= down]
        ahead = [(-d, 2) for d in (2 * stage - 1, 2 * stage) if d + 2 <= up]
        return ahead + [(d, -2) for d in (2 * stage - 1, 2 * stage) if d + 2 <= down]

    def fresh(stage):
        seen = (2 * stage - 1, 2 * stage)
        return [-d for d in seen if d <= up] + [d for d in seen if d <= down]

    def useful(k, distance, upward):
        return k + distance < nz if upward else k < down - (down - distance) % 2

    def k_wait(stage):
        for offset in fresh(stage):
            k = lax.rem(z + offset + nz, nz)

            @pl.when(useful(k, abs(offset), offset < 0))
            def _():
                remote(kv.at[k], kv.at[k], k_s.at[0], k_r.at[k], sib).wait_recv()

    def k_moves(stage):
        for i, (offset, step) in enumerate(reach(stage)):
            k = lax.rem(z + offset + nz, nz)
            src = k_ref if stage == 0 else kv.at[k]
            copy = remote(src, kv.at[k], k_s.at[4 * stage + i], k_r.at[k], zz(step + nz))
            yield useful(k, abs(offset) + abs(step), step > 0), copy

    def k_send(stage):
        for wanted, copy in k_moves(stage):
            pl.when(wanted)(copy.start)

    def k_pass(stage):
        k_wait(stage)
        if stage < stages:
            k_send(stage)

    stages = (nz // 2 + 1) // 2
    def ka_copy(peer):
        return remote(kaux.at[z], kaux.at[z], ka_s.at[peer], ka_r.at[z], at(z=peer))

    def to_later(copy, steps):
        for r in steps:
            peer = lax.rem(z + r, nz)

            @pl.when(peer > z)
            def _():
                copy(peer).start()

    for r in range(1, nb):
        remote(aux.at[b], aux.at[b], aux_s.at[r], aux_r.at[b], xc(r)).start()
    for i, (src, dst) in enumerate(sources):
        remote(src, dst.at[b], f_s.at[i, x], q_r.at[i, b], sib).start()
    for r in xorder:
        peer = lax.rem(x + r, nx)
        for i, (src, dst) in enumerate(sources):
            remote(src, dst.at[b], q_s.at[i, peer], q_r.at[i, b], at(x=peer)).start()
    k_send(0)

    def prepare(k):
        qt = qg[k].T
        dt = dg[k].T
        stats = jnp.concatenate([stat[k], jnp.zeros((TOK - 8, TOK), F32)], 0).T
        qtl[k] = jnp.concatenate([qt[64 * h : 64 * h + 64] for h in range(4)], 1)
        dtl[k] = jnp.concatenate([dt[64 * h : 64 * h + 64] for h in range(4)], 1)
        for r in range(8):
            rowb[r, k] = jnp.broadcast_to(stats[:, r : r + 1], (TOK, TOK))
        dq[k] = jnp.zeros((TOK, 256), F32)

    for r in range(1, nb):
        k = lax.rem(b + r, nb)
        remote(aux.at[k], aux.at[k], aux_s.at[r], aux_r.at[k], sib).wait_recv()
    before = jnp.zeros((4, TOK), F32)
    mine = jnp.zeros((4, TOK), F32)
    for k in range(nb):
        mine = jnp.where(b == k, before, mine)
        stat[k, 0:4, :] = (aux[k, 4:8, :] + before) * LOG2E
        stat[k, 4:8, :] = aux[k, 8:12, :]
        before = before + jnp.broadcast_to(aux[k, 0:4, TOK - 1 : TOK], (4, TOK))
    kaux[z, 0:4, :] = run + mine
    kaux[z, 4:8, :] = before
    ck[z, 0:4, :] = (run + mine) * LOG2E
    to_later(ka_copy, zorder)
    k_pass(1)
    for r in range(1, ny):
        remote(norm_ref, norm_all.at[y], n_s.at[r], n_r.at[y], yy(r)).start()
    prepare(b)

    def arrived(k):
        for i, (_, dst) in enumerate(sources):
            remote(dst.at[k], dst.at[k], q_s.at[i, 0], q_r.at[i, k], sib).wait_recv()

    arrived(2 * x + 1 - c)
    prepare(2 * x + 1 - c)
    for r in xorder:
        other = lax.rem(x + nx - r, nx)
        k = 2 * other + c
        arrived(k)
        for i, (_, dst) in enumerate(sources):
            remote(dst.at[k], dst.at[k], f_s.at[i, other], q_r.at[i, k], sib).start()
        prepare(k)
    for r in xorder:
        k = 2 * lax.rem(x + nx - r, nx) + 1 - c
        arrived(k)
        prepare(k)

    def offsets(i, total):
        k = z - 1 - i
        remote(kaux.at[k], kaux.at[k], ka_s.at[0], ka_r.at[k], sib).wait_recv()
        total = total + kaux[k, 4:8, :]
        ck[k, 0:4, :] = (kaux[k, 0:4, :] - total) * LOG2E
        return total

    even = lax.rem(z, 2) == 1
    skip = jnp.where(even, 0, 1)
    straight = jnp.minimum(nz - 1 - z, z)

    def visit(s):
        t = s - straight
        far = jnp.where(lax.rem(t, 2) == 1, z - straight - (t + 1) // 2, t // 2 - 1)
        return jnp.where(s <= straight, z - s, far)

    near = 6 - skip

    def turn(s):
        return visit(jnp.where(s < near, s, z + near - s))

    lane2 = lax.broadcasted_iota(jnp.int32, (TOK, TOK), 1)
    zero = jnp.zeros((64, TOK), BF16)

    def load_keys(blocks):
        for i, k in enumerate(blocks):
            block = kv[k]
            t = block.T
            cols = slice(i * TOK, (i + 1) * TOK)
            ktile[0, :, cols] = jnp.concatenate([t[:64], zero], 0)
            ktile[1, :, cols] = jnp.concatenate([zero, t[:64]], 0)
            vtile[0, :, cols] = jnp.concatenate([t[64:], zero], 0)
            vtile[1, :, cols] = jnp.concatenate([zero, t[64:]], 0)
            rolled = pltpu.roll(block.astype(F32), 64, 1).astype(BF16)
            none = jnp.zeros_like(block)
            kcat[i * TOK : (i + 1) * TOK, :] = jnp.where(lane2 < 64, block, none)
            kcat[2 * TOK + i * TOK : 2 * TOK + (i + 1) * TOK, :] = jnp.where(lane2 >= 64, rolled, none)

    def run_tile(blocks, first, between):
        load_keys(blocks)
        dkvt[...] = jnp.zeros((TOK, 2 * TOK), F32)
        cks = [jnp.concatenate([ck[k, h : h + 1, :] for k in blocks], 1) for h in range(4)]
        if first:
            col = lax.broadcasted_iota(jnp.int32, (TQ, 2 * TOK), 1)
            other = jnp.where(even, -1, 1 << 20)
            key_pos = jnp.where(col < TOK, b * TOK + col, other)

        def rows(t, _):
            q = qg[pl.ds(tb * t, tb)].reshape(TQ, 256)
            do = dg[pl.ds(tb * t, tb)].reshape(TQ, 256)
            ps, dss = [], []
            if first:
                allowed = key_pos <= lax.broadcasted_iota(jnp.int32, (TQ, 2 * TOK), 0) + t * TQ
            for h in range(4):
                lanes = slice(128 * (h // 2), 128 * (h // 2) + 128)
                s = jnp.dot(q[:, lanes], ktile[h % 2], preferred_element_type=F32)
                ra = rowb[h, pl.ds(tb * t, tb)].reshape(TQ, TOK)
                rd = rowb[4 + h, pl.ds(tb * t, tb)].reshape(TQ, TOK)
                logits = (s * c1 + jnp.concatenate([ra, ra], 1)) - cks[h]
                if first:
                    logits = jnp.where(allowed, logits, NEG_LARGE)
                p = jnp.exp2(logits)
                dp = jnp.dot(do[:, lanes], vtile[h % 2], preferred_element_type=F32)
                ds = p * (dp - jnp.concatenate([rd, rd], 1))
                ps.append(p.astype(BF16))
                dss.append(ds.astype(BF16))

            def by_block(parts):
                return jnp.concatenate([p[j * TOK : (j + 1) * TOK] for j in range(tb) for p in parts], 0)

            qt = jnp.concatenate([qtl[tb * t + j] for j in range(tb)], 1)
            dt = jnp.concatenate([dtl[tb * t + j] for j in range(tb)], 1)
            dkvt[:64] += jnp.dot(qt, by_block(dss), preferred_element_type=F32)
            dkvt[64:] += jnp.dot(dt, by_block(ps), preferred_element_type=F32)
            for g in range(2):
                pair = jnp.concatenate([dss[2 * g], dss[2 * g + 1]], 1)
                add = jnp.dot(pair, kcat[...], preferred_element_type=F32)
                dq[pl.ds(tb * t, tb), :, 128 * g : 128 * g + 128] += add.reshape(tb, TOK, TOK)
            return 0

        lax.fori_loop(0, nt // 2, rows, 0)
        between()
        lax.fori_loop(nt // 2, nt, rows, 0)

    def g_copy(k):
        return remote(gsend.at[k], grecv.at[z], g_s.at[k], g_r.at[z], at(z=k))

    def pass_on(i, k):
        gsend[k] = dkvt[:, i * TOK : (i + 1) * TOK].T.astype(BF16)
        g_copy(k).start()

    second = jnp.where(even, visit(1), z)
    early = jnp.minimum(z, 1)
    total = lax.fori_loop(0, early, offsets, jnp.zeros((4, TOK), F32))

    run_tile((z, second), True, lambda: k_pass(2) if stages > 1 else None)
    own[...] = dkvt[:, :TOK].T

    @pl.when(even)
    def _():
        pass_on(1, second)

    def later(i, carry):
        known, total = carry
        last = 2 * i + 1 - skip
        need = jnp.where(last <= jnp.minimum(straight, near - 1), last, z)
        total = lax.fori_loop(known, need, offsets, total)
        blocks = (turn(last - 1), turn(last))
        if stages > 3:
            pl.when(i == 3)(functools.partial(k_wait, 4))
        run_tile(blocks, False, lambda: pl.when(i == 1)(lambda: k_pass(3)) if stages > 2 else None)
        for j, k in enumerate(blocks):
            pass_on(j, k)
        return (need, total)

    lax.fori_loop(1, (z + 2) // 2, later, (early, total))
    if stages > 2:
        pl.when((z + 2) // 2 < 2)(functools.partial(k_pass, 3))
    if stages > 3:
        pl.when((z + 2) // 2 < 4)(functools.partial(k_wait, 4))

    for r in xorder + [0]:
        k = lax.rem(x + r, nx)
        slot = 2 * k + 1 - c
        remote(dq.at[slot], dqd.at[k], d_s.at[k], d_r.at[k], sib).start()
    for r in xorder:
        k = lax.rem(x + r, nx)
        remote(dqd.at[k], dqd.at[k], d_s.at[k], d_r.at[k], sib).wait_recv()
        dqs[k] = ((dq[2 * k + c] + dqd[k]) * 0.125).astype(BF16)
        remote(dqs.at[k], dqr.at[x], e_s.at[k], e_r.at[x], at(x=k)).start()
    remote(dqd.at[x], dqd.at[x], d_s.at[x], d_r.at[x], sib).wait_recv()

    for r in range(1, ny):
        k = lax.rem(y + r, ny)
        remote(norm_all.at[k], norm_all.at[k], n_s.at[r], n_r.at[k], sib).wait_recv()

    def collect(k, _):
        remote(grecv.at[k], grecv.at[k], g_s.at[0], g_r.at[k], sib).wait_recv()
        own[...] += grecv[k].astype(F32)
        return 0

    lax.fori_loop(z + 1, nz, collect, 0)
    kg = (own[:, :64] * 0.125).astype(BF16)
    both = own[...].T
    k_out[...] = (both[:64] * 0.125).astype(BF16)
    v_out[...] = both[64:].astype(BF16)

    width = norm_in.shape[1]
    rows16 = w_out.shape[0]
    half = rows16 // 2
    zs = width // (nb * rows16)
    for k in range(ny):
        w = jnp.dot(norm_all[k].T, kg, preferred_element_type=F32).reshape(zs * nb, rows16, 64)
        w = jnp.concatenate([w[:, :half], w[:, half:]], 2).reshape(zs, nx, 2, half, TOK)
        for cc in range(2):
            for xx in range(nx):
                part[cc, xx, k * zs : (k + 1) * zs] = w[:, xx, cc]
    h_copy = remote(part.at[1 - c], hrecv, h_s, h_r, sib)
    h_copy.start()
    h_copy.wait_recv()
    for r in xorder:
        k = lax.rem(x + r, nx)
        msend[k] = (part[c, k] + hrecv[k]).reshape(nz * half, TOK).astype(BF16)
        remote(msend.at[k], mrecv.at[x], m_s.at[k], m_r.at[x], at(x=k)).start()
    sums = part[c, x] + hrecv[x]
    for r in xorder:
        k = lax.rem(x + r, nx)
        remote(mrecv.at[k], mrecv.at[k], m_s.at[k], m_r.at[k], sib).wait_recv()
        sums = sums + mrecv[k].astype(F32).reshape(nz, half, TOK)
    mid[...] = sums

    def l_copy(k):
        return remote(mid.at[k], lrecv.at[z], l_s.at[k], l_r.at[z], at(z=k))

    for r in zorder[::-1]:
        l_copy(lax.rem(z + r, nz)).start()

    grad = (dq[b] + dqd[x]) * 0.125
    for r in xorder:
        k = lax.rem(x + r, nx)
        remote(dqr.at[k], dqr.at[k], e_s.at[k], e_r.at[k], sib).wait_recv()
        grad = grad + dqr[k].astype(F32)
    dq_out[...] = grad.astype(BF16)

    w_sum = mid[z]
    for r in zorder:
        k = lax.rem(z + r, nz)
        remote(lrecv.at[k], lrecv.at[k], l_s.at[k], l_r.at[k], sib).wait_recv()
        w_sum = w_sum + lrecv[k]
    w_out[...] = jnp.concatenate([w_sum[:, :64], w_sum[:, 64:]], 0)

    for r in range(1, nb):
        remote(aux.at[b], aux.at[b], aux_s.at[r], aux_r.at[b], xc(r)).wait_send()
    for i, (src, dst) in enumerate(sources):
        for k in range(nx):
            remote(src, dst.at[b], f_s.at[i, k], q_r.at[i, b], sib).wait_send()
        for r in xorder:
            peer = lax.rem(x + r, nx)
            remote(src, dst.at[b], q_s.at[i, peer], q_r.at[i, b], at(x=peer)).wait_send()
    for r in range(1, ny):
        remote(norm_ref, norm_all.at[y], n_s.at[r], n_r.at[y], yy(r)).wait_send()

    for stage in range(stages):
        for wanted, copy in k_moves(stage):
            pl.when(wanted)(copy.wait_send)

    def sent_on(k, _):
        ka_copy(k).wait_send()
        return 0

    lax.fori_loop(z + 1, nz, sent_on, 0)

    def sent_back(k, _):
        g_copy(k).wait_send()
        return 0

    lax.fori_loop(0, z, sent_back, 0)
    for k in range(nx):
        remote(dq.at[0], dqd.at[k], d_s.at[k], d_r.at[k], sib).wait_send()
    h_copy.wait_send()
    for r in xorder:
        k = lax.rem(x + r, nx)
        remote(dqs.at[k], dqr.at[x], e_s.at[k], e_r.at[x], at(x=k)).wait_send()
        remote(msend.at[k], mrecv.at[x], m_s.at[k], m_r.at[x], at(x=k)).wait_send()
    for r in zorder:
        l_copy(lax.rem(z + r, nz)).wait_send()


def attention(nz, nx, ny, *arrays):
    nb = 2 * nx
    vmem = pl.BlockSpec(memory_space=pltpu.VMEM)
    anywhere = pl.BlockSpec(memory_space=pltpu.HBM)
    dma = pltpu.SemaphoreType.DMA
    width = arrays[-1].shape[1]
    rows = ny * width // (nb * nz)
    bf, f32 = (lambda *s: pltpu.VMEM(s, BF16)), (lambda *s: pltpu.VMEM(s, F32))
    scratch = [
        bf(TOK, 256), bf(64, TOK), bf(64, TOK), f32(4, TOK), f32(4, TOK), bf(TOK, 256), bf(TOK, 256),
        bf(TOK, width), bf(TOK, TOK),
        bf(nb, TOK, 256), bf(nb, TOK, 256), bf(nz, TOK, TOK),
        f32(nb, 16, TOK), f32(nb, 8, TOK), f32(nz, 8, TOK), f32(nz, 8, TOK),
        f32(8, nb, TOK, TOK), bf(nb, 64, 4 * TOK), bf(nb, 64, 4 * TOK),
        bf(2, TOK, 2 * TOK), bf(2, TOK, 2 * TOK), bf(4 * TOK, TOK),
        f32(nb, TOK, 256), f32(TOK, 2 * TOK), f32(TOK, TOK),
        bf(nz, TOK, TOK), bf(nz, TOK, TOK),
        f32(nx, TOK, 256), bf(nx, TOK, 256), bf(nx, TOK, 256),
        bf(ny, TOK, width),
        f32(2, nx, nz, rows // 2, TOK), f32(nx, nz, rows // 2, TOK),
        bf(nx, nz * rows // 2, TOK), bf(nx, nz * rows // 2, TOK),
        f32(nz, rows // 2, TOK), f32(nz, rows // 2, TOK),
        dma((8,)),
        dma((nb,)), dma((nb,)),
        dma((2, nx)), dma((2, nb)), dma((2, nx)),
        dma((16,)), dma((nz,)), dma((nz,)), dma((nz,)),
        dma((ny,)), dma((ny,)),
        dma((nz,)), dma((nz,)),
        dma((nx,)), dma((nx,)), dma((nx,)), dma((nx,)),
        dma, dma,
        dma((nx,)), dma((nx,)),
        dma((nz,)), dma((nz,)),
    ]
    return pl.pallas_call(
        functools.partial(attention_kernel, nz, nx, ny),
        out_shape=(
            jax.ShapeDtypeStruct((TOK, 256), BF16),
            jax.ShapeDtypeStruct((64, TOK), BF16),
            jax.ShapeDtypeStruct((64, TOK), BF16),
            jax.ShapeDtypeStruct((rows, 64), F32),
        ),
        in_specs=[anywhere] * 8,
        out_specs=(vmem, vmem, vmem, vmem),
        scratch_shapes=scratch,
        compiler_params=pltpu.CompilerParams(
            collective_id=0, has_side_effects=True, vmem_limit_bytes=67043328
        ),
        name="attention",
    )(*arrays)


def finish_kernel(n, *refs):
    src, dst, held, sem = refs[:n], refs[n : 2 * n], refs[2 * n : 3 * n], refs[-1]
    loads = [pltpu.make_async_copy(src[i], held[i], sem.at[0, i]) for i in range(n)]
    stores = [pltpu.make_async_copy(held[i], dst[i], sem.at[1, i]) for i in range(n)]
    for load in loads:
        load.start()
    for load, store in zip(loads, stores):
        load.wait()
        store.start()
    for store in stores:
        store.wait()


def finish(*arrays):
    n = len(arrays)
    hbm = pl.BlockSpec(memory_space=pltpu.HBM)
    return pl.pallas_call(
        functools.partial(finish_kernel, n),
        out_shape=tuple(jax.ShapeDtypeStruct(a.shape, a.dtype) for a in arrays),
        in_specs=[hbm] * n,
        out_specs=(hbm,) * n,
        scratch_shapes=[pltpu.VMEM(a.shape, a.dtype) for a in arrays] + [pltpu.SemaphoreType.DMA((2, n))],
        compiler_params=pltpu.CompilerParams(vmem_limit_bytes=67043328),
        name="finish",
    )(*arrays)


def body(nz, nx, ny, q, k, v, *arrays):
    query_grad, key_grad, value_grad, weight_grad = finish(*attention(nz, nx, ny, q, k.T, v.T, *arrays))
    return (query_grad, key_grad.T, value_grad.T, weight_grad)


def solution(mesh):
    nz, nx, ny = mesh.shape["sp"] // 8, 4, mesh.shape["tp"]
    split = Mesh(mesh.devices.reshape(nz, nx, 2, ny), SP + ("tp",))
    placed = (
        P(SP, "tp"), P(SP, "tp"), P(SP, "tp"), P("tp", SP),
        P("tp", SP), P(SP, "tp"), P(SP, "tp"), P(SP, "tp"),
    )
    return jax.shard_map(
        functools.partial(body, nz, nx, ny),
        mesh=split,
        in_specs=placed,
        out_specs=(P(SP, "tp"), P(SP, "tp"), P(SP, "tp"), P(SP, "tp")),
        check_vma=False,
    )
```

```python
import functools
import math

import jax
import jax.numpy as jnp
from jax import lax
from jax.experimental import pallas as pl
from jax.experimental.pallas import tpu as pltpu
from jax.sharding import Mesh
from jax.sharding import PartitionSpec as P

SP = ("sp_0", "sp_1", "sp_2")
MESH = pl.DeviceIdType.MESH
LOG2E = math.log2(math.e)
NEG_LARGE = -1e30
TOK = 128
TQ = 512
F32, BF16 = jnp.float32, jnp.bfloat16


def at(z=None, x=None, c=None, y=None):
    named = {"sp_0": z, "sp_1": x, "sp_2": c, "tp": y}
    return {k: v for k, v in named.items() if v is not None}


def remote(src, dst, send, recv, peer):
    return pltpu.make_async_remote_copy(
        src_ref=src, dst_ref=dst, send_sem=send, recv_sem=recv, device_id=peer, device_id_type=MESH
    )


def attention_kernel(
    nz, nx, ny,
    q_in, k_in, v_in, gate_in, lse_in, out_in, do_in, norm_in,
    dq_hbm, k_hbm, v_hbm, w_hbm,
    dq_out, k_out, v_out, w_out,
    q_ref, k_half, v_half, gate_ref, lse_ref, out_ref, do_ref, norm_ref, k_ref,
    qg, dg, kv, aux, stat, kaux, ck, rowb, qtl, dtl, ktile, vtile, kcat, dq, dkvt, own,
    gsend, grecv, dqd, dqs, dqr, norm_all, part, hrecv, msend, mrecv, mid, lrecv,
    i_s, aux_s, aux_r, q_s, q_r, w_s, f_s, k_s, k_r, ka_s, ka_r, n_s, n_r, g_s, g_r, d_s, d_r, e_s, e_r,
    h_s, h_r, m_s, m_r, l_s, l_r, o_s,
):
    z, x, c, y = (lax.axis_index(a) for a in ("sp_0", "sp_1", "sp_2", "tp"))
    nb = 2 * nx
    b = 2 * x + c
    sib = at(c=1 - c)
    c1 = 0.125 * LOG2E
    tb = TQ // TOK
    nt = nb // tb

    def xc(r):
        k = lax.rem(b + r, nb)
        return at(x=k // 2, c=lax.rem(k, 2))

    def zz(r):
        return at(z=lax.rem(z + r, nz))

    def yy(r):
        return at(y=lax.rem(y + r, ny))

    loads = [
        pltpu.make_async_copy(src, dst, i_s.at[i])
        for i, (src, dst) in enumerate((
            (gate_in, gate_ref), (lse_in, lse_ref), (out_in, out_ref), (do_in, do_ref),
            (k_in, k_half), (v_in, v_half), (q_in, q_ref), (norm_in, norm_ref),
        ))
    ]
    for load in loads:
        load.start()
    peers = [xc(r) for r in range(1, nb)] + [zz(r) for r in range(1, nz)] + [yy(r) for r in range(1, ny)]
    barrier = pltpu.get_barrier_semaphore()
    for peer in peers:
        pl.semaphore_signal(barrier, inc=1, device_id=peer, device_id_type=MESH)
    for load in loads:
        load.wait()

    lane = lax.broadcasted_iota(jnp.int32, (4, TOK), 1)
    run = gate_ref[...]
    for s in (1, 2, 4, 8, 16, 32, 64):
        run = run + jnp.where(lane >= s, pltpu.roll(run, s, 1), 0.0)
    prod = (out_ref[...].astype(F32) * do_ref[...].astype(F32)).T
    aux[b, 0:4, :] = run
    aux[b, 4:8, :] = run - lse_ref[...]
    aux[b, 8:12, :] = jnp.sum(prod.reshape(4, 64, TOK), axis=1)
    aux[b, 12:16, :] = jnp.zeros((4, TOK), F32)
    k_ref[...] = jnp.concatenate([k_half[...], v_half[...]], axis=0).T
    kv[z] = k_ref[...]
    qg[b] = q_ref[...]
    dg[b] = do_ref[...]
    norm_all[y] = norm_ref[...]

    pl.semaphore_wait(barrier, len(peers))

    def nearest_first(n):
        pairs = zip(range(1, n // 2 + 1), range(n - 1, n // 2 - 1, -1))
        return list(dict.fromkeys(r for pair in pairs for r in pair))

    xorder, zorder = nearest_first(nx), nearest_first(nz)
    sources = ((q_ref, qg), (do_ref, dg))

    up, down = nz // 2, nz - 1 - nz // 2

    def reach(stage):
        if stage == 0:
            return [(0, d) for d in range(1, 5) if d <= up] + [(0, -d) for d in range(1, 5) if d <= down]
        ahead = [(-d, 2) for d in (2 * stage - 1, 2 * stage) if d + 2 <= up]
        return ahead + [(d, -2) for d in (2 * stage - 1, 2 * stage) if d + 2 <= down]

    def fresh(stage):
        seen = (2 * stage - 1, 2 * stage)
        return [-d for d in seen if d <= up] + [d for d in seen if d <= down]

    def useful(k, distance, upward):
        return k + distance < nz if upward else k < down - (down - distance) % 2

    def k_wait(stage):
        for offset in fresh(stage):
            k = lax.rem(z + offset + nz, nz)

            @pl.when(useful(k, abs(offset), offset < 0))
            def _():
                remote(kv.at[k], kv.at[k], k_s.at[0], k_r.at[k], sib).wait_recv()

    def k_moves(stage):
        for i, (offset, step) in enumerate(reach(stage)):
            k = lax.rem(z + offset + nz, nz)
            src = k_ref if stage == 0 else kv.at[k]
            copy = remote(src, kv.at[k], k_s.at[4 * stage + i if stage else i], k_r.at[k], zz(step + nz))
            yield useful(k, abs(offset) + abs(step), step > 0), copy

    def k_send(stage):
        for wanted, copy in k_moves(stage):
            pl.when(wanted)(copy.start)

    def k_pass(stage):
        k_wait(stage)
        if 1 < stage < stages:
            k_send(stage)

    stages = (nz // 2 + 1) // 2
    def ka_copy(peer):
        return remote(kaux.at[z], kaux.at[z], ka_s.at[peer], ka_r.at[z], at(z=peer))

    def to_later(copy, steps):
        for r in steps:
            peer = lax.rem(z + r, nz)

            @pl.when(peer > z)
            def _():
                copy(peer).start()

    for r in range(1, nb):
        remote(aux.at[b], aux.at[b], aux_s.at[r], aux_r.at[b], xc(r)).start()
    for i, (src, dst) in enumerate(sources):
        remote(src, dst.at[b], f_s.at[i, x], q_r.at[i, b], sib).start()
    def q_moves():
        for r in xorder:
            peer = lax.rem(x + r, nx)
            for i, (src, dst) in enumerate(sources[:1] if 2 * r == nx == 4 else sources):
                yield remote(src, dst.at[b], q_s.at[i, peer], q_r.at[i, b], at(x=peer))

    for copy in q_moves():
        copy.start()
    k_send(0)

    def prepare(k):
        qt = qg[k].T
        dt = dg[k].T
        stats = jnp.concatenate([stat[k], jnp.zeros((TOK - 8, TOK), F32)], 0).T
        qtl[k] = jnp.concatenate([qt[64 * h : 64 * h + 64] for h in range(4)], 1)
        dtl[k] = jnp.concatenate([dt[64 * h : 64 * h + 64] for h in range(4)], 1)
        for r in range(8):
            rowb[r, k] = jnp.broadcast_to(stats[:, r : r + 1], (TOK, TOK))
        dq[k] = jnp.zeros((TOK, 256), F32)

    for r in range(1, nb):
        k = lax.rem(b + r, nb)
        remote(aux.at[k], aux.at[k], aux_s.at[r], aux_r.at[k], sib).wait_recv()
    before = jnp.zeros((4, TOK), F32)
    mine = jnp.zeros((4, TOK), F32)
    for k in range(nb):
        mine = jnp.where(b == k, before, mine)
        stat[k, 0:4, :] = (aux[k, 4:8, :] + before) * LOG2E
        stat[k, 4:8, :] = aux[k, 8:12, :]
        before = before + jnp.broadcast_to(aux[k, 0:4, TOK - 1 : TOK], (4, TOK))
    kaux[z, 0:4, :] = run + mine
    kaux[z, 4:8, :] = before
    ck[z, 0:4, :] = (run + mine) * LOG2E
    to_later(ka_copy, zorder)
    for r in range(1, ny):
        remote(norm_ref, norm_all.at[y], n_s.at[r], n_r.at[y], yy(r)).start()
    prepare(b)

    def arrived(k):
        for i, (_, dst) in enumerate(sources):
            remote(dst.at[k], dst.at[k], q_s.at[i, 0], q_r.at[i, k], sib).wait_recv()

    def share(chip):
        k = 2 * chip + c
        arrived(k)
        for i, (_, dst) in enumerate(sources):
            remote(dst.at[k], dst.at[k], f_s.at[i, chip], q_r.at[i, k], sib).start()

    def relay():
        k = 2 * lax.rem(x + 1, nx) + c
        return remote(dg.at[k], dg.at[k], w_s, q_r.at[1, k], at(x=lax.rem(x + nx - 1, nx)))

    def complete(chip):
        prepare(2 * chip + c)
        arrived(2 * chip + 1 - c)
        prepare(2 * chip + 1 - c)

    arrived(2 * x + 1 - c)
    prepare(2 * x + 1 - c)
    odd = lax.rem(x, 2)
    if nx > 1:
        share(lax.rem(x + 1, nx))
    if nx == 4:
        relay().start()
        share(lax.rem(x + nx - 1, nx))
    if nx > 1:
        complete(x + 1 - 2 * odd)

    def rest():
        if nx == 4:
            complete(lax.rem(x + 3 - 2 * odd, nx))
            share(lax.rem(x + 2, nx))
            complete(lax.rem(x + 2, nx))
        if stages > 1:
            k_pass(2)

    def offsets(i, total):
        k = z - 1 - i
        remote(kaux.at[k], kaux.at[k], ka_s.at[0], ka_r.at[k], sib).wait_recv()
        total = total + kaux[k, 4:8, :]
        ck[k, 0:4, :] = (kaux[k, 0:4, :] - total) * LOG2E
        return total

    even = lax.rem(z, 2) == 1
    skip = jnp.where(even, 0, 1)
    straight = jnp.minimum(nz - 1 - z, z)

    def visit(s):
        t = s - straight
        far = jnp.where(lax.rem(t, 2) == 1, z - straight - (t + 1) // 2, t // 2 - 1)
        return jnp.where(s <= straight, z - s, far)

    held = jnp.where(z >= max(3 * nz // 4, 7), 2, 0)
    near = 8 - skip
    last_wait = jnp.where(even & (held == 0), 3, 4)

    def turn(s):
        ahead = jnp.where(s < near, s + held, z + near - s)
        return visit(jnp.where(s > z - held, z + 2 - skip - s, ahead))

    lane2 = lax.broadcasted_iota(jnp.int32, (TOK, TOK), 1)
    zero = jnp.zeros((64, TOK), BF16)

    def load_keys(blocks):
        for i, k in enumerate(blocks):
            block = kv[k]
            t = block.T
            cols = slice(i * TOK, (i + 1) * TOK)
            ktile[0, :, cols] = jnp.concatenate([t[:64], zero], 0)
            ktile[1, :, cols] = jnp.concatenate([zero, t[:64]], 0)
            vtile[0, :, cols] = jnp.concatenate([t[64:], zero], 0)
            vtile[1, :, cols] = jnp.concatenate([zero, t[64:]], 0)
            rolled = pltpu.roll(block.astype(F32), 64, 1).astype(BF16)
            none = jnp.zeros_like(block)
            kcat[i * TOK : (i + 1) * TOK, :] = jnp.where(lane2 < 64, block, none)
            kcat[2 * TOK + i * TOK : 2 * TOK + (i + 1) * TOK, :] = jnp.where(lane2 >= 64, rolled, none)

    def run_tile(blocks, first, between=None):
        load_keys(blocks)
        dkvt[...] = jnp.zeros((TOK, 2 * TOK), F32)
        cks = [jnp.concatenate([ck[k, h : h + 1, :] for k in blocks], 1) for h in range(4)]
        if first:
            col = lax.broadcasted_iota(jnp.int32, (TQ, 2 * TOK), 1)
            other = jnp.where(even, -1, 1 << 20)
            key_pos = jnp.where(col < TOK, b * TOK + col, other)

        def rows(t, _):
            q = qg[pl.ds(tb * t, tb)].reshape(TQ, 256)
            do = dg[pl.ds(tb * t, tb)].reshape(TQ, 256)
            ps, dss = [], []
            if first:
                allowed = key_pos <= lax.broadcasted_iota(jnp.int32, (TQ, 2 * TOK), 0) + t * TQ
            for h in range(4):
                lanes = slice(128 * (h // 2), 128 * (h // 2) + 128)
                s = jnp.dot(q[:, lanes], ktile[h % 2], preferred_element_type=F32)
                ra = rowb[h, pl.ds(tb * t, tb)].reshape(TQ, TOK)
                rd = rowb[4 + h, pl.ds(tb * t, tb)].reshape(TQ, TOK)
                logits = (s * c1 + jnp.concatenate([ra, ra], 1)) - cks[h]
                if first:
                    logits = jnp.where(allowed, logits, NEG_LARGE)
                p = jnp.exp2(logits)
                dp = jnp.dot(do[:, lanes], vtile[h % 2], preferred_element_type=F32)
                ds = p * (dp - jnp.concatenate([rd, rd], 1))
                ps.append(p.astype(BF16))
                dss.append(ds.astype(BF16))

            def by_block(parts):
                return jnp.concatenate([p[j * TOK : (j + 1) * TOK] for j in range(tb) for p in parts], 0)

            qt = jnp.concatenate([qtl[tb * t + j] for j in range(tb)], 1)
            dt = jnp.concatenate([dtl[tb * t + j] for j in range(tb)], 1)
            dkvt[:64] += jnp.dot(qt, by_block(dss), preferred_element_type=F32)
            dkvt[64:] += jnp.dot(dt, by_block(ps), preferred_element_type=F32)
            for g in range(2):
                pair = jnp.concatenate([dss[2 * g], dss[2 * g + 1]], 1)
                add = jnp.dot(pair, kcat[...], preferred_element_type=F32)
                dq[pl.ds(tb * t, tb), :, 128 * g : 128 * g + 128] += add.reshape(tb, TOK, TOK)
            return 0

        if between is None:
            lax.fori_loop(0, nt, rows, 0)
        else:
            lax.fori_loop(0, nt // 2, lambda i, _: rows(x // 2, 0), 0)
            between()
            lax.fori_loop(nt // 2, nt, lambda i, _: rows(nt // 2 - x // 2 if nt == 2 else i, 0), 0)

    def g_copy(k):
        return remote(gsend.at[k], grecv.at[z], g_s.at[k], g_r.at[z], at(z=k))

    def pass_on(i, k):
        gsend[k] = dkvt[:, i * TOK : (i + 1) * TOK].T.astype(BF16)
        g_copy(k).start()

    k_pass(1)

    second = jnp.where(even, visit(1), z)
    early = jnp.minimum(z, 1)
    total = lax.fori_loop(0, early, offsets, jnp.zeros((4, TOK), F32))

    run_tile((z, second), True, rest)
    own[...] = dkvt[:, :TOK].T

    @pl.when(even)
    def _():
        pass_on(1, second)

    def later(i, carry):
        known, total = carry
        last = 2 * i + 1 - skip
        need = jnp.where((last <= jnp.minimum(straight, near - 1)) & (held == 0), last, z)
        total = lax.fori_loop(known, need, offsets, total)
        blocks = (turn(last - 1), turn(last))
        if stages > 2:
            pl.when(i == 2)(functools.partial(k_pass, 3))
        if stages > 3:
            pl.when(i == last_wait)(functools.partial(k_wait, 4))
        run_tile(blocks, False)
        for j, k in enumerate(blocks):
            pass_on(j, k)
        return (need, total)

    lax.fori_loop(1, (z + 2) // 2, later, (early, total))
    if stages > 2:
        pl.when((z + 2) // 2 < 3)(functools.partial(k_pass, 3))
    if stages > 3:
        pl.when((z + 2) // 2 <= last_wait)(functools.partial(k_wait, 4))

    for r in xorder + [0]:
        k = lax.rem(x + r, nx)
        slot = 2 * k + 1 - c
        remote(dq.at[slot], dqd.at[k], d_s.at[k], d_r.at[k], sib).start()
    for r in xorder:
        k = lax.rem(x + r, nx)
        remote(dqd.at[k], dqd.at[k], d_s.at[k], d_r.at[k], sib).wait_recv()
        dqs[k] = ((dq[2 * k + c] + dqd[k]) * 0.125).astype(BF16)
        remote(dqs.at[k], dqr.at[x], e_s.at[k], e_r.at[x], at(x=k)).start()
    remote(dqd.at[x], dqd.at[x], d_s.at[x], d_r.at[x], sib).wait_recv()

    for r in range(1, ny):
        k = lax.rem(y + r, ny)
        remote(norm_all.at[k], norm_all.at[k], n_s.at[r], n_r.at[k], sib).wait_recv()

    def collect(k, _):
        remote(grecv.at[k], grecv.at[k], g_s.at[0], g_r.at[k], sib).wait_recv()
        own[...] += grecv[k].astype(F32)
        return 0

    lax.fori_loop(z + 1, nz, collect, 0)
    kg = (own[:, :64] * 0.125).astype(BF16)
    both = own[...].T
    k_out[...] = (both[:64] * 0.125).astype(BF16)
    v_out[...] = both[64:].astype(BF16)
    held_out = ((k_out, k_hbm), (v_out, v_hbm), (dq_out, dq_hbm), (w_out, w_hbm))
    stores = [pltpu.make_async_copy(src, dst, o_s.at[i]) for i, (src, dst) in enumerate(held_out)]
    stores[0].start()
    stores[1].start()

    width = norm_in.shape[1]
    rows16 = w_out.shape[0]
    half = rows16 // 2
    zs = width // (nb * rows16)
    for k in range(ny):
        w = jnp.dot(norm_all[k].T, kg, preferred_element_type=F32).reshape(zs * nb, rows16, 64)
        w = jnp.concatenate([w[:, :half], w[:, half:]], 2).reshape(zs, nx, 2, half, TOK)
        for cc in range(2):
            for xx in range(nx):
                part[cc, xx, k * zs : (k + 1) * zs] = w[:, xx, cc]
    h_copy = remote(part.at[1 - c], hrecv, h_s, h_r, sib)
    h_copy.start()
    h_copy.wait_recv()
    for r in xorder:
        k = lax.rem(x + r, nx)
        msend[k] = (part[c, k] + hrecv[k]).reshape(nz * half, TOK).astype(BF16)
        remote(msend.at[k], mrecv.at[x], m_s.at[k], m_r.at[x], at(x=k)).start()
    sums = part[c, x] + hrecv[x]
    for r in xorder:
        k = lax.rem(x + r, nx)
        remote(mrecv.at[k], mrecv.at[k], m_s.at[k], m_r.at[k], sib).wait_recv()
        sums = sums + mrecv[k].astype(F32).reshape(nz, half, TOK)
    mid[...] = sums

    def l_copy(k):
        return remote(mid.at[k], lrecv.at[z], l_s.at[k], l_r.at[z], at(z=k))

    for r in zorder[::-1]:
        l_copy(lax.rem(z + r, nz)).start()

    grad = (dq[b] + dqd[x]) * 0.125
    for r in xorder:
        k = lax.rem(x + r, nx)
        remote(dqr.at[k], dqr.at[k], e_s.at[k], e_r.at[k], sib).wait_recv()
        grad = grad + dqr[k].astype(F32)
    dq_out[...] = grad.astype(BF16)
    stores[2].start()

    w_sum = mid[z]
    for r in zorder:
        k = lax.rem(z + r, nz)
        remote(lrecv.at[k], lrecv.at[k], l_s.at[k], l_r.at[k], sib).wait_recv()
        w_sum = w_sum + lrecv[k]
    w_out[...] = jnp.concatenate([w_sum[:, :64], w_sum[:, 64:]], 0)
    stores[3].start()

    for r in range(1, nb):
        remote(aux.at[b], aux.at[b], aux_s.at[r], aux_r.at[b], xc(r)).wait_send()
    for i, (src, dst) in enumerate(sources):
        for k in range(nx):
            remote(src, dst.at[b], f_s.at[i, k], q_r.at[i, b], sib).wait_send()
    for copy in q_moves():
        copy.wait_send()
    if nx == 4:
        relay().wait_send()
    for r in range(1, ny):
        remote(norm_ref, norm_all.at[y], n_s.at[r], n_r.at[y], yy(r)).wait_send()

    for stage in range(stages):
        for wanted, copy in k_moves(stage) if stage != 1 else ():
            pl.when(wanted)(copy.wait_send)

    def sent_on(k, _):
        ka_copy(k).wait_send()
        return 0

    lax.fori_loop(z + 1, nz, sent_on, 0)

    def sent_back(k, _):
        g_copy(k).wait_send()
        return 0

    lax.fori_loop(0, z, sent_back, 0)
    for k in range(nx):
        remote(dq.at[0], dqd.at[k], d_s.at[k], d_r.at[k], sib).wait_send()
    h_copy.wait_send()
    for r in xorder:
        k = lax.rem(x + r, nx)
        remote(dqs.at[k], dqr.at[x], e_s.at[k], e_r.at[x], at(x=k)).wait_send()
        remote(msend.at[k], mrecv.at[x], m_s.at[k], m_r.at[x], at(x=k)).wait_send()
    for r in zorder:
        l_copy(lax.rem(z + r, nz)).wait_send()
    for store in stores:
        store.wait()


def attention(nz, nx, ny, *arrays):
    nb = 2 * nx
    anywhere = pl.BlockSpec(memory_space=pltpu.HBM)
    dma = pltpu.SemaphoreType.DMA
    width = arrays[-1].shape[1]
    rows = ny * width // (nb * nz)
    bf, f32 = (lambda *s: pltpu.VMEM(s, BF16)), (lambda *s: pltpu.VMEM(s, F32))
    scratch = [
        bf(TOK, 256), bf(64, TOK), bf(64, TOK), f32(rows, 64),
        bf(TOK, 256), bf(64, TOK), bf(64, TOK), f32(4, TOK), f32(4, TOK), bf(TOK, 256), bf(TOK, 256),
        bf(TOK, width), bf(TOK, TOK),
        bf(nb, TOK, 256), bf(nb, TOK, 256), bf(nz, TOK, TOK),
        f32(nb, 16, TOK), f32(nb, 8, TOK), f32(nz, 8, TOK), f32(nz, 8, TOK),
        f32(8, nb, TOK, TOK), bf(nb, 64, 4 * TOK), bf(nb, 64, 4 * TOK),
        bf(2, TOK, 2 * TOK), bf(2, TOK, 2 * TOK), bf(4 * TOK, TOK),
        f32(nb, TOK, 256), f32(TOK, 2 * TOK), f32(TOK, TOK),
        bf(nz, TOK, TOK), bf(nz, TOK, TOK),
        f32(nx, TOK, 256), bf(nx, TOK, 256), bf(nx, TOK, 256),
        bf(ny, TOK, width),
        f32(2, nx, nz, rows // 2, TOK), f32(nx, nz, rows // 2, TOK),
        bf(nx, nz * rows // 2, TOK), bf(nx, nz * rows // 2, TOK),
        f32(nz, rows // 2, TOK), f32(nz, rows // 2, TOK),
        dma((8,)),
        dma((nb,)), dma((nb,)),
        dma((2, nx)), dma((2, nb)), dma, dma((2, nx)),
        dma((16,)), dma((nz,)), dma((nz,)), dma((nz,)),
        dma((ny,)), dma((ny,)),
        dma((nz,)), dma((nz,)),
        dma((nx,)), dma((nx,)), dma((nx,)), dma((nx,)),
        dma, dma,
        dma((nx,)), dma((nx,)),
        dma((nz,)), dma((nz,)),
        dma((4,)),
    ]
    return pl.pallas_call(
        functools.partial(attention_kernel, nz, nx, ny),
        out_shape=(
            jax.ShapeDtypeStruct((TOK, 256), BF16),
            jax.ShapeDtypeStruct((64, TOK), BF16),
            jax.ShapeDtypeStruct((64, TOK), BF16),
            jax.ShapeDtypeStruct((rows, 64), F32),
        ),
        in_specs=[anywhere] * 8,
        out_specs=(anywhere,) * 4,
        scratch_shapes=scratch,
        compiler_params=pltpu.CompilerParams(
            collective_id=0, has_side_effects=True, vmem_limit_bytes=67043328
        ),
        name="attention",
    )(*arrays)


def finish_kernel(n, *refs):
    src, dst, held, sem = refs[:n], refs[n : 2 * n], refs[2 * n : 3 * n], refs[-1]
    loads = [pltpu.make_async_copy(src[i], held[i], sem.at[0, i]) for i in range(n)]
    stores = [pltpu.make_async_copy(held[i], dst[i], sem.at[1, i]) for i in range(n)]
    for load in loads:
        load.start()
    for load, store in zip(loads, stores):
        load.wait()
        store.start()
    for store in stores:
        store.wait()


def finish(*arrays):
    n = len(arrays)
    hbm = pl.BlockSpec(memory_space=pltpu.HBM)
    return pl.pallas_call(
        functools.partial(finish_kernel, n),
        out_shape=tuple(jax.ShapeDtypeStruct(a.shape, a.dtype) for a in arrays),
        in_specs=[hbm] * n,
        out_specs=(hbm,) * n,
        scratch_shapes=[pltpu.VMEM(a.shape, a.dtype) for a in arrays] + [pltpu.SemaphoreType.DMA((2, n))],
        compiler_params=pltpu.CompilerParams(vmem_limit_bytes=67043328),
        name="finish",
    )(*arrays)


def body(nz, nx, ny, q, k, v, *arrays):
    query_grad, key_grad, value_grad, weight_grad = finish(*attention(nz, nx, ny, q, k.T, v.T, *arrays))
    return (query_grad, key_grad.T, value_grad.T, weight_grad)


def solution(mesh):
    nz, nx, ny = mesh.shape["sp"] // 8, 4, mesh.shape["tp"]
    split = Mesh(mesh.devices.reshape(nz, nx, 2, ny), SP + ("tp",))
    placed = (
        P(SP, "tp"), P(SP, "tp"), P(SP, "tp"), P("tp", SP),
        P("tp", SP), P(SP, "tp"), P(SP, "tp"), P(SP, "tp"),
    )
    return jax.shard_map(
        functools.partial(body, nz, nx, ny),
        mesh=split,
        in_specs=placed,
        out_specs=(P(SP, "tp"), P(SP, "tp"), P(SP, "tp"), P(SP, "tp")),
        check_vma=False,
    )
```

```python
import functools
import math

import jax
import jax.numpy as jnp
from jax import lax
from jax.experimental import pallas as pl
from jax.experimental.pallas import tpu as pltpu
from jax.sharding import Mesh
from jax.sharding import PartitionSpec as P

SP = ("sp_0", "sp_1", "sp_2")
MESH = pl.DeviceIdType.MESH
LOG2E = math.log2(math.e)
NEG_LARGE = -1e30
TOK = 128
TQ = 512
F32, BF16 = jnp.float32, jnp.bfloat16


def at(z=None, x=None, c=None, y=None):
    named = {"sp_0": z, "sp_1": x, "sp_2": c, "tp": y}
    return {k: v for k, v in named.items() if v is not None}


def remote(src, dst, send, recv, peer):
    return pltpu.make_async_remote_copy(
        src_ref=src, dst_ref=dst, send_sem=send, recv_sem=recv, device_id=peer, device_id_type=MESH
    )


def attention_kernel(
    nz, nx, ny,
    q_in, k_in, v_in, gate_in, lse_in, out_in, do_in, norm_in,
    dq_hbm, k_hbm, v_hbm, w_hbm,
    dq_out, k_out, v_out, w_out,
    q_ref, k_half, v_half, gate_ref, lse_ref, out_ref, do_ref, norm_ref, k_ref,
    qg, dg, kv, aux, stat, kaux, ck, rowb, qtl, dtl, ktile, vtile, kcat, dq, dkvt, own,
    gsend, grecv, dqd, dqs, dqr, norm_all, part, hrecv, msend, mrecv, mid, lrecv,
    i_s, aux_s, aux_r, q_s, q_r, w_s, f_s, k_s, k_r, ka_s, ka_r, n_s, n_r, g_s, g_r, d_s, d_r, e_s, e_r,
    h_s, h_r, m_s, m_r, l_s, l_r, o_s,
):
    z, x, c, y = (lax.axis_index(a) for a in ("sp_0", "sp_1", "sp_2", "tp"))
    nb = 2 * nx
    b = 2 * x + c
    sib = at(c=1 - c)
    c1 = 0.125 * LOG2E
    tb = TQ // TOK
    nt = nb // tb

    def xc(r):
        k = lax.rem(b + r, nb)
        return at(x=k // 2, c=lax.rem(k, 2))

    def zz(r):
        return at(z=lax.rem(z + r, nz))

    def yy(r):
        return at(y=lax.rem(y + r, ny))

    loads = [
        pltpu.make_async_copy(src, dst, i_s.at[i])
        for i, (src, dst) in enumerate((
            (gate_in, gate_ref), (lse_in, lse_ref), (out_in, out_ref), (do_in, do_ref),
            (k_in, k_half), (v_in, v_half), (q_in, q_ref), (norm_in, norm_ref),
        ))
    ]
    for load in loads:
        load.start()
    peers = [xc(r) for r in range(1, nb)] + [zz(r) for r in range(1, nz)] + [yy(r) for r in range(1, ny)]
    barrier = pltpu.get_barrier_semaphore()
    for peer in peers:
        pl.semaphore_signal(barrier, inc=1, device_id=peer, device_id_type=MESH)
    for load in loads:
        load.wait()

    lane = lax.broadcasted_iota(jnp.int32, (4, TOK), 1)
    run = gate_ref[...]
    for s in (1, 2, 4, 8, 16, 32, 64):
        run = run + jnp.where(lane >= s, pltpu.roll(run, s, 1), 0.0)
    prod = (out_ref[...].astype(F32) * do_ref[...].astype(F32)).T
    aux[b, 0:4, :] = run
    aux[b, 4:8, :] = run - lse_ref[...]
    aux[b, 8:12, :] = jnp.sum(prod.reshape(4, 64, TOK), axis=1)
    aux[b, 12:16, :] = jnp.zeros((4, TOK), F32)
    k_ref[...] = jnp.concatenate([k_half[...], v_half[...]], axis=0).T
    kv[z] = k_ref[...]
    qg[b] = q_ref[...]
    dg[b] = do_ref[...]
    norm_all[y] = norm_ref[...]

    pl.semaphore_wait(barrier, len(peers))

    def nearest_first(n):
        pairs = zip(range(1, n // 2 + 1), range(n - 1, n // 2 - 1, -1))
        return list(dict.fromkeys(r for pair in pairs for r in pair))

    xorder, zorder = nearest_first(nx), nearest_first(nz)
    sources = ((q_ref, qg), (do_ref, dg))

    up, down = nz // 2, nz - 1 - nz // 2

    def reach(stage):
        if stage == 0:
            return [(0, d) for d in range(1, 5) if d <= up] + [(0, -d) for d in range(1, 5) if d <= down]
        ahead = [(-d, 2) for d in (2 * stage - 1, 2 * stage) if d + 2 <= up]
        return ahead + [(d, -2) for d in (2 * stage - 1, 2 * stage) if d + 2 <= down]

    def fresh(stage):
        seen = (2 * stage - 1, 2 * stage)
        return [-d for d in seen if d <= up] + [d for d in seen if d <= down]

    def useful(k, distance, upward):
        return k + distance < nz if upward else k < down - (down - distance) % 2

    def k_wait(stage):
        for offset in fresh(stage):
            k = lax.rem(z + offset + nz, nz)

            @pl.when(useful(k, abs(offset), offset < 0))
            def _():
                remote(kv.at[k], kv.at[k], k_s.at[0], k_r.at[k], sib).wait_recv()

    def k_moves(stage):
        for i, (offset, step) in enumerate(reach(stage)):
            k = lax.rem(z + offset + nz, nz)
            src = k_ref if stage == 0 else kv.at[k]
            copy = remote(src, kv.at[k], k_s.at[4 * stage + i if stage else i], k_r.at[k], zz(step + nz))
            yield useful(k, abs(offset) + abs(step), step > 0), copy

    def k_send(stage):
        for wanted, copy in k_moves(stage):
            pl.when(wanted)(copy.start)

    def k_pass(stage):
        k_wait(stage)
        if 1 < stage < stages:
            k_send(stage)

    stages = (nz // 2 + 1) // 2
    def ka_copy(peer):
        return remote(kaux.at[z], kaux.at[z], ka_s.at[peer], ka_r.at[z], at(z=peer))

    def to_later(copy, steps):
        for r in steps:
            peer = lax.rem(z + r, nz)

            @pl.when(peer > z)
            def _():
                copy(peer).start()

    for r in range(1, nb):
        remote(aux.at[b], aux.at[b], aux_s.at[r], aux_r.at[b], xc(r)).start()
    for i, (src, dst) in enumerate(sources):
        remote(src, dst.at[b], f_s.at[i, x], q_r.at[i, b], sib).start()
    def q_moves():
        for r in xorder:
            peer = lax.rem(x + r, nx)
            for i, (src, dst) in enumerate(sources[:1] if 2 * r == nx == 4 else sources):
                yield remote(src, dst.at[b], q_s.at[i, peer], q_r.at[i, b], at(x=peer))

    for copy in q_moves():
        copy.start()
    k_send(0)

    def prepare(k):
        qt = qg[k].T
        dt = dg[k].T
        stats = jnp.concatenate([stat[k], jnp.zeros((TOK - 8, TOK), F32)], 0).T
        qtl[k] = jnp.concatenate([qt[64 * h : 64 * h + 64] for h in range(4)], 1)
        dtl[k] = jnp.concatenate([dt[64 * h : 64 * h + 64] for h in range(4)], 1)
        for r in range(8):
            rowb[r, k] = jnp.broadcast_to(stats[:, r : r + 1], (TOK, TOK))
        dq[k] = jnp.zeros((TOK, 256), F32)

    for r in range(1, nb):
        k = lax.rem(b + r, nb)
        remote(aux.at[k], aux.at[k], aux_s.at[r], aux_r.at[k], sib).wait_recv()
    before = jnp.zeros((4, TOK), F32)
    mine = jnp.zeros((4, TOK), F32)
    for k in range(nb):
        mine = jnp.where(b == k, before, mine)
        stat[k, 0:4, :] = (aux[k, 4:8, :] + before) * LOG2E
        stat[k, 4:8, :] = aux[k, 8:12, :]
        before = before + jnp.broadcast_to(aux[k, 0:4, TOK - 1 : TOK], (4, TOK))
    kaux[z, 0:4, :] = run + mine
    kaux[z, 4:8, :] = before
    ck[z, 0:4, :] = (run + mine) * LOG2E
    to_later(ka_copy, zorder)
    for r in range(1, ny):
        remote(norm_ref, norm_all.at[y], n_s.at[r], n_r.at[y], yy(r)).start()
    prepare(b)

    def arrived(k):
        for i, (_, dst) in enumerate(sources):
            remote(dst.at[k], dst.at[k], q_s.at[i, 0], q_r.at[i, k], sib).wait_recv()

    def share(chip):
        k = 2 * chip + c
        arrived(k)
        for i, (_, dst) in enumerate(sources):
            remote(dst.at[k], dst.at[k], f_s.at[i, chip], q_r.at[i, k], sib).start()

    def relay():
        k = 2 * lax.rem(x + 1, nx) + c
        return remote(dg.at[k], dg.at[k], w_s, q_r.at[1, k], at(x=lax.rem(x + nx - 1, nx)))

    def complete(chip):
        prepare(2 * chip + c)
        arrived(2 * chip + 1 - c)
        prepare(2 * chip + 1 - c)

    arrived(2 * x + 1 - c)
    prepare(2 * x + 1 - c)
    odd = lax.rem(x, 2)
    if nx > 1:
        share(lax.rem(x + 1, nx))
    if nx == 4:
        relay().start()
        share(lax.rem(x + nx - 1, nx))
    if nx > 1:
        complete(x + 1 - 2 * odd)

    def rest():
        if nx == 4:
            complete(lax.rem(x + 3 - 2 * odd, nx))
            share(lax.rem(x + 2, nx))
            complete(lax.rem(x + 2, nx))
        if stages > 1:
            k_pass(2)

    def offsets(i, total):
        k = z - 1 - i
        remote(kaux.at[k], kaux.at[k], ka_s.at[0], ka_r.at[k], sib).wait_recv()
        total = total + kaux[k, 4:8, :]
        ck[k, 0:4, :] = (kaux[k, 0:4, :] - total) * LOG2E
        return total

    even = lax.rem(z, 2) == 1
    skip = jnp.where(even, 0, 1)
    straight = jnp.minimum(nz - 1 - z, z)

    def visit(s):
        t = s - straight
        far = jnp.where(lax.rem(t, 2) == 1, z - straight - (t + 1) // 2, t // 2 - 1)
        return jnp.where(s <= straight, z - s, far)

    held = jnp.where(z >= max(3 * nz // 4, 7), 2, 0)
    near = 8 - skip
    last_wait = jnp.where(even & (held == 0), 3, 4)

    def turn(s):
        ahead = jnp.where(s < near, s + held, z + near - s)
        return visit(jnp.where(s > z - held, z + 2 - skip - s, ahead))

    lane2 = lax.broadcasted_iota(jnp.int32, (TOK, TOK), 1)
    zero = jnp.zeros((64, TOK), BF16)

    def load_keys(blocks):
        for i, k in enumerate(blocks):
            block = kv[k]
            t = block.T
            cols = slice(i * TOK, (i + 1) * TOK)
            ktile[0, :, cols] = jnp.concatenate([t[:64], zero], 0)
            ktile[1, :, cols] = jnp.concatenate([zero, t[:64]], 0)
            vtile[0, :, cols] = jnp.concatenate([t[64:], zero], 0)
            vtile[1, :, cols] = jnp.concatenate([zero, t[64:]], 0)
            rolled = pltpu.roll(block.astype(F32), 64, 1).astype(BF16)
            none = jnp.zeros_like(block)
            kcat[i * TOK : (i + 1) * TOK, :] = jnp.where(lane2 < 64, block, none)
            kcat[2 * TOK + i * TOK : 2 * TOK + (i + 1) * TOK, :] = jnp.where(lane2 >= 64, rolled, none)

    def run_tile(blocks, first, between=None):
        load_keys(blocks)
        dkvt[...] = jnp.zeros((TOK, 2 * TOK), F32)
        cks = [jnp.concatenate([ck[k, h : h + 1, :] for k in blocks], 1) for h in range(4)]
        if first:
            col = lax.broadcasted_iota(jnp.int32, (TQ, 2 * TOK), 1)
            other = jnp.where(even, -1, 1 << 20)
            key_pos = jnp.where(col < TOK, b * TOK + col, other)

        def rows(t, _):
            q = qg[pl.ds(tb * t, tb)].reshape(TQ, 256)
            do = dg[pl.ds(tb * t, tb)].reshape(TQ, 256)
            ps, dss = [], []
            if first:
                allowed = key_pos <= lax.broadcasted_iota(jnp.int32, (TQ, 2 * TOK), 0) + t * TQ
            for h in range(4):
                lanes = slice(128 * (h // 2), 128 * (h // 2) + 128)
                s = jnp.dot(q[:, lanes], ktile[h % 2], preferred_element_type=F32)
                ra = rowb[h, pl.ds(tb * t, tb)].reshape(TQ, TOK)
                rd = rowb[4 + h, pl.ds(tb * t, tb)].reshape(TQ, TOK)
                logits = (s * c1 + jnp.concatenate([ra, ra], 1)) - cks[h]
                if first:
                    logits = jnp.where(allowed, logits, NEG_LARGE)
                p = jnp.exp2(logits)
                dp = jnp.dot(do[:, lanes], vtile[h % 2], preferred_element_type=F32)
                ds = p * (dp - jnp.concatenate([rd, rd], 1))
                ps.append(p.astype(BF16))
                dss.append(ds.astype(BF16))

            def by_block(parts):
                return jnp.concatenate([p[j * TOK : (j + 1) * TOK] for j in range(tb) for p in parts], 0)

            qt = jnp.concatenate([qtl[tb * t + j] for j in range(tb)], 1)
            dt = jnp.concatenate([dtl[tb * t + j] for j in range(tb)], 1)
            dkvt[:64] += jnp.dot(qt, by_block(dss), preferred_element_type=F32)
            dkvt[64:] += jnp.dot(dt, by_block(ps), preferred_element_type=F32)
            for g in range(2):
                pair = jnp.concatenate([dss[2 * g], dss[2 * g + 1]], 1)
                add = jnp.dot(pair, kcat[...], preferred_element_type=F32)
                dq[pl.ds(tb * t, tb), :, 128 * g : 128 * g + 128] += add.reshape(tb, TOK, TOK)
            return 0

        if between is None:
            lax.fori_loop(0, nt, rows, 0)
        else:
            lax.fori_loop(0, nt // 2, lambda i, _: rows(x // 2, 0), 0)
            between()
            lax.fori_loop(nt // 2, nt, lambda i, _: rows(nt // 2 - x // 2 if nt == 2 else i, 0), 0)

    def g_copy(k):
        return remote(gsend.at[k], grecv.at[z], g_s.at[k], g_r.at[z], at(z=k))

    def pass_on(i, k):
        gsend[k] = dkvt[:, i * TOK : (i + 1) * TOK].T.astype(BF16)
        g_copy(k).start()

    k_pass(1)

    second = jnp.where(even, visit(1), z)
    early = jnp.minimum(z, 1)
    total = lax.fori_loop(0, early, offsets, jnp.zeros((4, TOK), F32))

    run_tile((z, second), True, rest)
    own[...] = dkvt[:, :TOK].T

    @pl.when(even)
    def _():
        pass_on(1, second)

    def later(i, carry):
        known, total = carry
        last = 2 * i + 1 - skip
        need = jnp.where((last <= jnp.minimum(straight, near - 1)) & (held == 0), last, z)
        total = lax.fori_loop(known, need, offsets, total)
        blocks = (turn(last - 1), turn(last))
        if stages > 2:
            pl.when(i == 2)(functools.partial(k_pass, 3))
        if stages > 3:
            pl.when(i == last_wait)(functools.partial(k_wait, 4))
        run_tile(blocks, False)
        for j, k in enumerate(blocks):
            pass_on(j, k)
        return (need, total)

    lax.fori_loop(1, (z + 2) // 2, later, (early, total))
    if stages > 2:
        pl.when((z + 2) // 2 < 3)(functools.partial(k_pass, 3))
    if stages > 3:
        pl.when((z + 2) // 2 <= last_wait)(functools.partial(k_wait, 4))

    for r in xorder + [0]:
        k = lax.rem(x + r, nx)
        slot = 2 * k + 1 - c
        remote(dq.at[slot], dqd.at[k], d_s.at[k], d_r.at[k], sib).start()
    for r in xorder:
        k = lax.rem(x + r, nx)
        remote(dqd.at[k], dqd.at[k], d_s.at[k], d_r.at[k], sib).wait_recv()
        dqs[k] = ((dq[2 * k + c] + dqd[k]) * 0.125).astype(BF16)
        remote(dqs.at[k], dqr.at[x], e_s.at[k], e_r.at[x], at(x=k)).start()
    remote(dqd.at[x], dqd.at[x], d_s.at[x], d_r.at[x], sib).wait_recv()

    for r in range(1, ny):
        k = lax.rem(y + r, ny)
        remote(norm_all.at[k], norm_all.at[k], n_s.at[r], n_r.at[k], sib).wait_recv()

    def collect(k, _):
        remote(grecv.at[k], grecv.at[k], g_s.at[0], g_r.at[k], sib).wait_recv()
        own[...] += grecv[k].astype(F32)
        return 0

    lax.fori_loop(z + 1, nz, collect, 0)
    kg = (own[:, :64] * 0.125).astype(BF16)
    both = own[...].T
    k_out[...] = (both[:64] * 0.125).astype(BF16)
    v_out[...] = both[64:].astype(BF16)
    held_out = ((k_out, k_hbm), (v_out, v_hbm), (dq_out, dq_hbm), (w_out, w_hbm))
    stores = [pltpu.make_async_copy(src, dst, o_s.at[i]) for i, (src, dst) in enumerate(held_out)]
    stores[0].start()
    stores[1].start()

    width = norm_in.shape[1]
    rows16 = w_out.shape[0]
    half = rows16 // 2
    zs = width // (nb * rows16)
    for k in range(ny):
        w = jnp.dot(norm_all[k].T, kg, preferred_element_type=F32).reshape(zs * nb, rows16, 64)
        w = jnp.concatenate([w[:, :half], w[:, half:]], 2).reshape(zs, nx, 2, half, TOK)
        for cc in range(2):
            for xx in range(nx):
                part[cc, xx, k * zs : (k + 1) * zs] = w[:, xx, cc]
    h_copy = remote(part.at[1 - c], hrecv, h_s, h_r, sib)
    h_copy.start()
    h_copy.wait_recv()
    for r in xorder:
        k = lax.rem(x + r, nx)
        msend[k] = (part[c, k] + hrecv[k]).reshape(nz * half, TOK).astype(BF16)
        remote(msend.at[k], mrecv.at[x], m_s.at[k], m_r.at[x], at(x=k)).start()
    sums = part[c, x] + hrecv[x]
    for r in xorder:
        k = lax.rem(x + r, nx)
        remote(mrecv.at[k], mrecv.at[k], m_s.at[k], m_r.at[k], sib).wait_recv()
        sums = sums + mrecv[k].astype(F32).reshape(nz, half, TOK)
    mid[...] = sums

    def l_copy(k):
        return remote(mid.at[k], lrecv.at[z], l_s.at[k], l_r.at[z], at(z=k))

    for r in zorder[::-1]:
        l_copy(lax.rem(z + r, nz)).start()

    grad = (dq[b] + dqd[x]) * 0.125
    for r in xorder:
        k = lax.rem(x + r, nx)
        remote(dqr.at[k], dqr.at[k], e_s.at[k], e_r.at[k], sib).wait_recv()
        grad = grad + dqr[k].astype(F32)
    dq_out[...] = grad.astype(BF16)
    stores[2].start()

    w_sum = mid[z]
    for r in zorder:
        k = lax.rem(z + r, nz)
        remote(lrecv.at[k], lrecv.at[k], l_s.at[k], l_r.at[k], sib).wait_recv()
        w_sum = w_sum + lrecv[k]
    w_out[...] = jnp.concatenate([w_sum[:, :64], w_sum[:, 64:]], 0)
    stores[3].start()

    for r in range(1, nb):
        remote(aux.at[b], aux.at[b], aux_s.at[r], aux_r.at[b], xc(r)).wait_send()
    for i, (src, dst) in enumerate(sources):
        for k in range(nx):
            remote(src, dst.at[b], f_s.at[i, k], q_r.at[i, b], sib).wait_send()
    for copy in q_moves():
        copy.wait_send()
    if nx == 4:
        relay().wait_send()
    for r in range(1, ny):
        remote(norm_ref, norm_all.at[y], n_s.at[r], n_r.at[y], yy(r)).wait_send()

    for stage in range(stages):
        for wanted, copy in k_moves(stage) if stage != 1 else ():
            pl.when(wanted)(copy.wait_send)

    def sent_on(k, _):
        ka_copy(k).wait_send()
        return 0

    lax.fori_loop(z + 1, nz, sent_on, 0)

    def sent_back(k, _):
        g_copy(k).wait_send()
        return 0

    lax.fori_loop(0, z, sent_back, 0)
    for k in range(nx):
        remote(dq.at[0], dqd.at[k], d_s.at[k], d_r.at[k], sib).wait_send()
    h_copy.wait_send()
    for r in xorder:
        k = lax.rem(x + r, nx)
        remote(dqs.at[k], dqr.at[x], e_s.at[k], e_r.at[x], at(x=k)).wait_send()
        remote(msend.at[k], mrecv.at[x], m_s.at[k], m_r.at[x], at(x=k)).wait_send()
    for r in zorder:
        l_copy(lax.rem(z + r, nz)).wait_send()
    for store in stores:
        store.wait()


def attention(nz, nx, ny, *arrays):
    nb = 2 * nx
    anywhere = pl.BlockSpec(memory_space=pltpu.HBM)
    dma = pltpu.SemaphoreType.DMA
    width = arrays[-1].shape[1]
    rows = ny * width // (nb * nz)
    bf, f32 = (lambda *s: pltpu.VMEM(s, BF16)), (lambda *s: pltpu.VMEM(s, F32))
    scratch = [
        bf(TOK, 256), bf(64, TOK), bf(64, TOK), f32(rows, 64),
        bf(TOK, 256), bf(64, TOK), bf(64, TOK), f32(4, TOK), f32(4, TOK), bf(TOK, 256), bf(TOK, 256),
        bf(TOK, width), bf(TOK, TOK),
        bf(nb, TOK, 256), bf(nb, TOK, 256), bf(nz, TOK, TOK),
        f32(nb, 16, TOK), f32(nb, 8, TOK), f32(nz, 8, TOK), f32(nz, 8, TOK),
        f32(8, nb, TOK, TOK), bf(nb, 64, 4 * TOK), bf(nb, 64, 4 * TOK),
        bf(2, TOK, 2 * TOK), bf(2, TOK, 2 * TOK), bf(4 * TOK, TOK),
        f32(nb, TOK, 256), f32(TOK, 2 * TOK), f32(TOK, TOK),
        bf(nz, TOK, TOK), bf(nz, TOK, TOK),
        f32(nx, TOK, 256), bf(nx, TOK, 256), bf(nx, TOK, 256),
        bf(ny, TOK, width),
        f32(2, nx, nz, rows // 2, TOK), f32(nx, nz, rows // 2, TOK),
        bf(nx, nz * rows // 2, TOK), bf(nx, nz * rows // 2, TOK),
        f32(nz, rows // 2, TOK), f32(nz, rows // 2, TOK),
        dma((8,)),
        dma((nb,)), dma((nb,)),
        dma((2, nx)), dma((2, nb)), dma, dma((2, nx)),
        dma((16,)), dma((nz,)), dma((nz,)), dma((nz,)),
        dma((ny,)), dma((ny,)),
        dma((nz,)), dma((nz,)),
        dma((nx,)), dma((nx,)), dma((nx,)), dma((nx,)),
        dma, dma,
        dma((nx,)), dma((nx,)),
        dma((nz,)), dma((nz,)),
        dma((4,)),
    ]
    return pl.pallas_call(
        functools.partial(attention_kernel, nz, nx, ny),
        out_shape=(
            jax.ShapeDtypeStruct((TOK, 256), BF16),
            jax.ShapeDtypeStruct((64, TOK), BF16),
            jax.ShapeDtypeStruct((64, TOK), BF16),
            jax.ShapeDtypeStruct((rows, 64), F32),
        ),
        in_specs=[anywhere] * 8,
        out_specs=(anywhere,) * 4,
        scratch_shapes=scratch,
        compiler_params=pltpu.CompilerParams(
            collective_id=0, has_side_effects=True, vmem_limit_bytes=67043328
        ),
        name="attention",
    )(*arrays)


def finish_kernel(n, *refs):
    sem = refs[-1]
    copies = [pltpu.make_async_copy(refs[i], refs[n + i], sem.at[i]) for i in range(n)]
    for copy in copies:
        copy.start()
    for copy in copies:
        copy.wait()


def finish(*arrays):
    n = len(arrays)
    hbm = pl.BlockSpec(memory_space=pltpu.HBM)
    return pl.pallas_call(
        functools.partial(finish_kernel, n),
        out_shape=tuple(jax.ShapeDtypeStruct(a.shape, a.dtype) for a in arrays),
        in_specs=[hbm] * n,
        out_specs=(hbm,) * n,
        scratch_shapes=[pltpu.SemaphoreType.DMA((n,))],
        compiler_params=pltpu.CompilerParams(vmem_limit_bytes=67043328),
        name="finish",
    )(*arrays)


def body(nz, nx, ny, q, k, v, *arrays):
    query_grad, key_grad, value_grad, weight_grad = finish(*attention(nz, nx, ny, q, k.T, v.T, *arrays))
    return (query_grad, key_grad.T, value_grad.T, weight_grad)


def solution(mesh):
    nz, nx, ny = mesh.shape["sp"] // 8, 4, mesh.shape["tp"]
    split = Mesh(mesh.devices.reshape(nz, nx, 2, ny), SP + ("tp",))
    placed = (
        P(SP, "tp"), P(SP, "tp"), P(SP, "tp"), P("tp", SP),
        P("tp", SP), P(SP, "tp"), P(SP, "tp"), P(SP, "tp"),
    )
    return jax.shard_map(
        functools.partial(body, nz, nx, ny),
        mesh=split,
        in_specs=placed,
        out_specs=(P(SP, "tp"), P(SP, "tp"), P(SP, "tp"), P(SP, "tp")),
        check_vma=False,
    )
```
